512 devices in a mesh: ep: 32 (over z, core), tp: 16 (over y, x).
Axes of the slice: x: 4, y: 4, z: 16, core: 2. Of those that a mesh axis runs over, the one named last changes fastest.
Arguments:
- query_maps: bfloat16 [4096, 16, 128], P('ep', 'tp'), may hold values from -6 to 6
- key_maps: bfloat16 [4096, 16, 128], P('ep', 'tp'), may hold values from -6 to 6
- value_rows: bfloat16 [4096, 16, 128], P('ep', 'tp'), may hold values from -6 to 6
- head_lambda: float32 [16], P('tp'), may hold values from 0.3 to 0.8
- head_gain: float32 [128], replicated, may hold values from 0.1 to 1.9
- out_weight: bfloat16 [2048, 2048], P('tp'), may hold values from -0.125 to 0.125
- token_rows: bfloat16 [4096, 2048], P('ep'), may hold values from -36 to 36
- norm_gain: float32 [2048], replicated, may hold values from 0.1 to 1.9
- expert_ids: int32 [4096, 4], P('ep'), may hold values from 0 to 31, all different within a row; in each aligned block of 128 rows (0 to 127, 128 to 255, ...) at most 20 rows name the same one
- route_weights: float32 [4096, 4], P('ep'), may hold values from 0.1 to 0.5
- gate_weight: bfloat16 [32, 2048, 4096], P('ep', None, 'tp'), may hold values from -0.82864076 to 0.82864076
- up_weight: bfloat16 [32, 2048, 4096], P('ep', None, 'tp'), may hold values from -0.82864076 to 0.82864076
- down_weight: bfloat16 [32, 4096, 2048], P('ep', 'tp'), may hold values from -0.03125 to 0.03125
Outputs:
- mixed_rows: bfloat16 [4096, 2048], P(('ep', 'tp'))
- mixed_experts: bfloat16 [4096, 2048], P('ep', 'tp')
The draws below stay inside these ranges and needn't reach their ends.
Inputs may be any that keep to these rules, and one draw needn't show every extreme that they name: `expert_ids`: each row names 4 different experts. Among the rows of one index of ep no expert is named more than 20 times, and in every draw some expert is named exactly 20 times there.
All inputs are finite; a program needn't handle non-finite values.
Results may differ from the reference program's by a relative error of at most 0.015.
Values may be sent and summed in bfloat16 or wider, within the bound.
A program may use at most 64 MiB of HBM per device.

```python
import math
import jax
import jax.numpy as jnp
import numpy as np
from jax import lax

D = 2048
HEADS = 16
HEAD_DIM = 64
FF = 4096
TOPK = 4
TOKB_DEV = 128
EXPERTS = 32
TOKA = 4096
TOKB = 4096
CAP = 20
N_EP = 32
N_TP = 16


def score_pair(key):
    parts = jax.random.split(jax.random.fold_in(key, 11), 3)
    full_shape = (TOKA, HEADS, 2 * HEAD_DIM)
    query_vals = jnp.clip(1.3 * jax.random.normal(parts[1], full_shape, jnp.float32), -6.0, 6.0)
    key_vals = jnp.clip(1.3 * jax.random.normal(parts[2], full_shape, jnp.float32), -6.0, 6.0)
    return (query_vals.astype(jnp.bfloat16), key_vals.astype(jnp.bfloat16))


def draw_query_maps(key, part):
    return score_pair(key)[0]


def draw_key_maps(key, part):
    return score_pair(key)[1]


def draw_token_rows(key, part):
    parts = jax.random.split(jax.random.fold_in(key, 23), 3)
    row_scales = jnp.exp(jax.random.uniform(parts[0], (TOKB, 1), jnp.float32, math.log(0.3), math.log(3.0)))
    values = jnp.clip(jax.random.normal(parts[1], (TOKB, D), jnp.float32), -4.0, 4.0)
    col_scales = jnp.exp(jax.random.uniform(parts[2], (1, D), jnp.float32, math.log(0.3), math.log(3.0)))
    return (values * row_scales * col_scales).astype(jnp.bfloat16)


def expert_matrix(key, salt_value):
    parts = jax.random.split(jax.random.fold_in(key, salt_value), 1)
    full_shape = (EXPERTS, D, FF)
    values = jnp.clip(jax.random.normal(parts[0], full_shape, jnp.float32), -6.0, 6.0) * (2.5 * D ** (-0.5))
    return values.astype(jnp.bfloat16)


def draw_gate_weight(key, part):
    return expert_matrix(key, 31)


def draw_up_weight(key, part):
    return expert_matrix(key, 37)


def block_levels(own_key, shape, shards, smallest, high):
    def one(axis_at, shards_of):
        heights = jax.random.uniform(jax.random.fold_in(jax.random.fold_in(own_key, 6), axis_at), (shards_of,), jnp.float32, smallest / len(shards), high / len(shards))
        return jnp.repeat(jnp.exp(heights), shape[axis_at] // shards_of).reshape((-1,) + (1,) * (len(shape) - axis_at - 1))

    gain = one(*shards[0])
    for cut in shards[1:]:
        gain = gain * one(*cut)
    return gain


def assign_block(stream_key, own, number, rows, number_of, top, limit, lean):
    ranking = jax.random.permutation(stream_key, number_of)
    crowded, common = load_shares(number_of, rows * top, limit, lean, True), load_shares(number_of, rows * top, limit, lean, False)
    places = jnp.arange(number_of)

    def named(sizes, rotation):
        used = int((sizes > 0).sum())
        fixed = max(1, used // 4)
        moved = fixed + (places - fixed + rotation * (used - fixed)) % max(1, number_of - fixed)
        return jnp.zeros((number_of,), jnp.int32).at[ranking[jnp.where(places < fixed, places, moved)]].set(jnp.asarray(sizes, jnp.int32))

    sizes = jnp.where(number % 4 == 0, named(crowded, number // 4), named(common, number - number // 4 - 1))
    mixed = jax.random.permutation(jax.random.fold_in(own, 3), number_of)
    giver, receiver = mixed[0:number_of // 2 * 2:2], mixed[1:number_of // 2 * 2:2]
    margin = jnp.minimum(sizes[giver] - 1, limit - sizes[receiver]) // 2
    margin = jnp.where((giver == ranking[0]) | (receiver == ranking[0]) | (sizes[receiver] == 0), 0, jnp.maximum(margin, 0))
    moved = jax.random.randint(jax.random.fold_in(own, 4), (number_of // 2,), 0, 1 << 20) % (margin + 1)
    sizes = sizes.at[giver].add(-moved).at[receiver].add(moved)
    members = jnp.searchsorted(jnp.cumsum(sizes), jnp.arange(rows * top), side="right").astype(jnp.int32)
    table = members.reshape(top, rows).T
    table = table[jax.random.permutation(jax.random.fold_in(own, 1), rows)]
    rotation = jax.random.randint(jax.random.fold_in(own, 2), (rows, 1), 0, top)
    return jnp.take_along_axis(table, (jnp.arange(top)[None, :] + rotation) % top, axis=1)


def load_shares(number_of, total, limit, lean, full):
    loads = [(1 << 20) // math.isqrt(rank ** lean) + 1 for rank in range(1, number_of + 1)]
    largest = limit if full else min(limit, max(-(-total // number_of), total * loads[0] // sum(loads)))
    least = 1 if total - largest >= number_of - 1 else 0
    given, spare = [largest] + [least] * (number_of - 1), total - largest - least * (number_of - 1)
    while spare > 0:
        movable = [i for i in range(1, number_of) if given[i] < largest] or [i for i in range(1, number_of) if given[i] < limit]
        mass, left = sum([loads[i] for i in movable]), spare
        for i in movable:
            extra = min(limit - given[i], max(1, left * loads[i] // mass), spare)
            given[i] = given[i] + extra
            spare = spare - extra
    return np.array(given)


def scatter_about(stream_key, dims, width, most, cuts=(), kind=jnp.bfloat16):
    entries = width * jax.random.normal(stream_key, dims, jnp.float32)
    if cuts:
        entries = entries * block_levels(stream_key, dims, cuts, -0.22, 0.18)
    return jnp.clip(entries, -most, most).astype(kind)


def setup_inputs(seed: int = 0) -> dict:
    keys = jax.random.split(jax.random.key(seed), 14)
    query_maps = draw_query_maps(jax.random.fold_in(keys[13], 71), 0)
    key_maps = draw_key_maps(jax.random.fold_in(keys[13], 71), 0)
    value_rows = scatter_about(keys[2], (TOKA, HEADS, 2 * HEAD_DIM), 1.0, 6.0, ((0, 32), (1, 16)))
    head_lambda = jnp.clip(0.3 + 0.5 * jax.random.uniform(keys[3], (HEADS,), jnp.float32) ** block_levels(keys[3], (HEADS,), ((0, 16),), -0.2, 0.2), 0.3, 0.8)
    head_gain = jnp.clip(1.0 + 0.18 * jax.random.normal(keys[4], (2 * HEAD_DIM,), jnp.float32), 0.1, 1.9)
    out_weight = scatter_about(keys[5], (HEADS * 2 * HEAD_DIM, D), (HEADS * 2 * HEAD_DIM) ** -0.5, 0.125, ((0, 16),))
    token_rows = draw_token_rows(jax.random.fold_in(keys[13], 71), 0)
    norm_gain = jnp.clip(1.0 + 0.18 * jax.random.normal(keys[7], (D,), jnp.float32), 0.1, 1.9)
    expert_ids_keys = jax.random.split(jax.random.fold_in(keys[8], 1), TOKB // TOKB_DEV)
    expert_ids_turns = jax.random.permutation(jax.random.fold_in(keys[8], 3), TOKB // TOKB_DEV)
    expert_ids = jax.vmap(lambda own, number: assign_block(jax.random.fold_in(keys[8], 2), own, number, TOKB_DEV, EXPERTS, TOPK, CAP, 1))(expert_ids_keys, expert_ids_turns).reshape((TOKB, TOPK))
    route_weights = jnp.clip(0.1 + 0.4 * jax.random.uniform(keys[9], (TOKB, TOPK), jnp.float32) ** block_levels(keys[9], (TOKB, TOPK), ((0, 32),), -0.2, 0.2), 0.1, 0.5)
    gate_weight = draw_gate_weight(jax.random.fold_in(keys[13], 71), 0)
    up_weight = draw_up_weight(jax.random.fold_in(keys[13], 71), 0)
    down_weight = scatter_about(keys[12], (EXPERTS, FF, D), (8 * FF) ** -0.5, 0.03125, ((0, 32), (1, 16)))
    return dict(query_maps=query_maps, key_maps=key_maps, value_rows=value_rows, head_lambda=head_lambda, head_gain=head_gain, out_weight=out_weight, token_rows=token_rows, norm_gain=norm_gain, expert_ids=expert_ids, route_weights=route_weights, gate_weight=gate_weight, up_weight=up_weight, down_weight=down_weight)


NORM_EPS = 1e-05
CLAMP_LIMIT = 7.0
GATE_SLOPE = 1.702

def rounded(values):
    return lax.optimization_barrier(values.astype(jnp.bfloat16)).astype(jnp.float32)

def mixer_half(query_maps, key_maps, value_rows, head_lambda, head_gain, out_weight):
    head_width = HEAD_DIM
    score_scale = head_width ** (-0.5)
    block_len = math.gcd(TOKA, 256)
    key_float = key_maps.astype(jnp.float32)
    value_float = value_rows.astype(jnp.float32)
    outputs = []
    for begin_at in range(0, TOKA, block_len):
        ending = begin_at + block_len
        query_float = query_maps[begin_at:ending].astype(jnp.float32)
        query_pos = begin_at + jnp.arange(block_len, dtype=jnp.int32)
        key_pos = jnp.arange(ending, dtype=jnp.int32)
        causal = key_pos[None, :] <= query_pos[:, None]
        results = []
        for map_index in range(2):
            col_low = map_index * head_width
            col_high = col_low + head_width
            scores = jnp.einsum('qhd,khd->hqk', query_float[:, :, col_low:col_high], key_float[:ending, :, col_low:col_high]) * score_scale
            scores = jnp.where(causal[None], scores, -jnp.inf)
            row_max = lax.optimization_barrier(jnp.max(scores, axis=-1, keepdims=True))
            exp_terms = jnp.exp(scores - row_max)
            denominator = lax.optimization_barrier(jnp.sum(exp_terms, axis=-1))
            weights = rounded(exp_terms)
            numerator = jnp.einsum('hqk,khd->qhd', weights, value_float[:ending])
            results.append(numerator / jnp.transpose(denominator)[:, :, None])
        attended = results[0] - head_lambda[None, :, None] * results[1]
        mean_sq = lax.optimization_barrier(jnp.mean(attended * attended, axis=-1, keepdims=True))
        normed = attended * lax.rsqrt(mean_sq + NORM_EPS) * head_gain
        outputs.append(normed.astype(jnp.bfloat16))
    head_rows = jnp.concatenate(outputs, axis=0).reshape(TOKA, HEADS * 2 * HEAD_DIM)
    group_width = HEADS * 2 * HEAD_DIM // N_TP
    summed = jnp.zeros((TOKA, D), jnp.float32)
    for group_index in range(N_TP):
        group_rows = head_rows[:, group_index * group_width:(group_index + 1) * group_width]
        group_weight = out_weight[group_index * group_width:(group_index + 1) * group_width]
        summed = summed + rounded(jnp.dot(group_rows, group_weight, preferred_element_type=jnp.float32))
    return summed.astype(jnp.bfloat16)

def expert_half(token_rows, norm_gain, expert_ids, route_weights, gate_weight, up_weight, down_weight):
    rows_float = token_rows.astype(jnp.float32)
    mean_sq = lax.optimization_barrier(jnp.mean(rows_float * rows_float, axis=-1, keepdims=True))
    normed = (rows_float * lax.rsqrt(mean_sq + NORM_EPS) * norm_gain).astype(jnp.bfloat16)
    flat_ids = expert_ids.reshape(N_EP, TOKB_DEV * TOPK)
    onehot = (flat_ids[:, :, None] == jnp.arange(EXPERTS, dtype=jnp.int32)[None, None, :]).astype(jnp.int32)
    rank_before = jnp.cumsum(onehot, axis=1) - onehot
    slot_of = lax.optimization_barrier(jnp.sum(rank_before * onehot, axis=2)).astype(jnp.int32)
    sources = jnp.arange(N_EP, dtype=jnp.int32)[:, None]
    token_of = sources * TOKB_DEV + jnp.arange(TOKB_DEV * TOPK, dtype=jnp.int32)[None, :] // TOPK
    row_index = sources * CAP + slot_of
    slot_table = jnp.full((EXPERTS, N_EP * CAP), TOKB, jnp.int32).at[flat_ids, row_index].set(token_of)
    padded = jnp.concatenate([normed, jnp.zeros((1, D), jnp.bfloat16)], axis=0)

    def one_expert(inputs):
        row_ids, gate_matrix, up_matrix, down_matrix = inputs
        chosen = padded[row_ids]
        gate_pre = jnp.dot(chosen, gate_matrix, preferred_element_type=jnp.float32)
        up_pre = jnp.dot(chosen, up_matrix, preferred_element_type=jnp.float32)
        gated = jnp.minimum(gate_pre, CLAMP_LIMIT)
        clipped = jnp.clip(up_pre, -CLAMP_LIMIT, CLAMP_LIMIT)
        active = rounded((clipped + 1.0) * gated * jax.nn.sigmoid(GATE_SLOPE * gated))
        grouped = active.reshape(N_EP * CAP, N_TP, FF // N_TP)
        down_grouped = down_matrix.astype(jnp.float32).reshape(N_TP, FF // N_TP, D)
        terms = jnp.einsum('rgf,gfd->rgd', grouped, down_grouped)
        return lax.optimization_barrier(jnp.sum(rounded(terms), axis=1)).astype(jnp.bfloat16)
    expert_out = lax.map(one_expert, (slot_table, gate_weight, up_weight, down_weight))
    picked = expert_out[flat_ids.reshape(-1), row_index.reshape(-1)].astype(jnp.float32)
    combined = lax.optimization_barrier(jnp.sum(picked.reshape(TOKB, TOPK, D) * route_weights[:, :, None], axis=1))
    return combined.astype(jnp.bfloat16)

def reference(query_maps, key_maps, value_rows, head_lambda, head_gain, out_weight, token_rows, norm_gain, expert_ids, route_weights, gate_weight, up_weight, down_weight):
    mixed_rows = mixer_half(query_maps, key_maps, value_rows, head_lambda, head_gain, out_weight)
    mixed_experts = expert_half(token_rows, norm_gain, expert_ids, route_weights, gate_weight, up_weight, down_weight)
    return (mixed_rows, mixed_experts)
```

```python
import functools

import jax
import jax.numpy as jnp
import numpy as np
from jax import lax
from jax.experimental import pallas as pl
from jax.experimental.pallas import tpu as pltpu
from jax.sharding import PartitionSpec as P

NORM_EPS = 1e-05
CLAMP_LIMIT = 7.0
GATE_SLOPE = 1.702
MESH = pl.DeviceIdType.MESH

EP, TP, SIDE, CHIPS = 32, 16, 4, 16
CAP, SLAB = 20, 24
ROWS, HALF = EP * CAP, EP * CAP // 2
PADDED, PAD_HALF = EP * SLAB, EP * SLAB // 2
D, LANE, TOK, UNITS = 2048, 128, 128, 256
BAND = SIDE * LANE
TILE = 160
F32, BF16 = jnp.float32, jnp.bfloat16
NN = (((1,), (0,)), ((), ()))
NT = (((1,), (1,)), ((), ()))


def mm(a, b, dims=NN):
    return lax.dot_general(a, b, dims, preferred_element_type=F32)


def slot_tables():
    rows = np.arange(PADDED)
    spread = np.zeros((PADDED, LANE), np.float32)
    spread[rows, rows // SLAB] = 1.0
    spread[rows, EP] = -(rows % SLAB)
    pack = np.zeros((HALF, PAD_HALF), np.float32)
    r = np.arange(HALF)
    pack[r, r // CAP * SLAB + r % CAP] = 1.0
    return spread, pack, pack.T.copy()


def kernel(
    qkv_ref, lam_ref, gain_ref, ow_hbm, tok_ref, ngain_ref, ids_ref, wts_ref, spread_ref, pack_ref, unpack_ref,
    gate_hbm, up_hbm, down_hbm,
    rows_ref, experts_ref,
    kv, m_ref, l_ref, acc_ref, psend, prec, xsend, xrec, xall, ypart, rs1a, rs1b, z0, z1, rs2a, rs2b, rsend, rrec,
    ow_ref, gate_ref, up_ref, down_ref,
    local_sem, plus_s, plus_r, minus_s, minus_r, sib_s, sib_r, p_s, p_r, d_s, d_r, ag1_s, ag1_r, ag2_s, ag2_r,
    r1_s, r1_r, r2_s, r2_r, b_s, b_r,
):
    ep = lax.axis_index("ep")
    tp = lax.axis_index("tp")
    z, core = ep // 2, ep % 2
    x, y = tp % SIDE, tp // SIDE
    sib = z * 2 + (1 - core)

    def lanes(block, width=LANE):
        return pl.ds(pl.multiple_of(block * width, width), width)

    def remote(src, dst, ssem, rsem, e, t):
        return pltpu.make_async_remote_copy(
            src_ref=src, dst_ref=dst, send_sem=ssem, recv_sem=rsem, device_id=(e, t), device_id_type=MESH
        )

    def x_peer(j):
        return y * SIDE + (x + j) % SIDE

    def y_peer(j):
        return ((y + j) % SIDE) * SIDE + x

    barrier = pltpu.get_barrier_semaphore()

    def greet_ep(i, carry):
        pl.semaphore_signal(barrier, inc=1, device_id=((ep + i) % EP, tp), device_id_type=MESH)
        return carry

    def greet_tp(i, carry):
        pl.semaphore_signal(barrier, inc=1, device_id=(ep, (tp + i) % TP), device_id_type=MESH)
        return carry

    lax.fori_loop(1, EP, greet_ep, 0)
    lax.fori_loop(1, TP, greet_tp, 0)

    weight_copies = [
        pltpu.make_async_copy(src, dst, local_sem.at[i])
        for i, (src, dst) in enumerate(((gate_hbm, gate_ref), (up_hbm, up_ref), (down_hbm, down_ref), (ow_hbm, ow_ref)))
    ]
    for copy in weight_copies:
        copy.start()

    tokens = tok_ref[...].astype(F32)
    scale = lax.rsqrt(jnp.mean(tokens * tokens, axis=-1, keepdims=True) + NORM_EPS)
    mine = tok_ref[:, lanes(tp)].astype(F32)
    normed = (mine * scale * ngain_ref[:, lanes(tp)]).astype(BF16)
    expert = lax.broadcasted_iota(jnp.int32, (TOK, LANE), 1)
    token = lax.broadcasted_iota(jnp.int32, (TOK, LANE), 0)
    named = jnp.zeros((TOK, LANE), F32)
    weight = jnp.zeros((TOK, LANE), F32)
    for k in range(4):
        hit = ids_ref[:, k : k + 1] == expert
        named = named + jnp.where(hit, 1.0, 0.0)
        weight = weight + jnp.where(hit, wts_ref[:, k : k + 1], 0.0)
    before = jnp.where(expert < token, 1.0, 0.0).astype(BF16)
    rank = mm(before, named.astype(BF16))
    place = jnp.where(named > 0.5, rank, -1.0)
    place = jnp.where(expert < EP, place, jnp.where(expert == EP, 1.0, 0.0))
    spread = spread_ref[...]
    chosen = mm(spread, jnp.transpose(place).astype(BF16))
    chosen = jnp.where(jnp.abs(chosen) < 0.5, 1.0, 0.0).astype(BF16)
    outgoing = mm(chosen, normed).astype(BF16)
    for e in range(EP):
        xsend[e] = outgoing[e * SLAB : (e + 1) * SLAB]
    kv[ep] = qkv_ref[1:3]

    pl.semaphore_wait(barrier, EP - 1 + TP - 1)

    def dispatch(i):
        peer = (ep + i) % EP
        return remote(xsend.at[peer], xrec.at[ep], d_s.at[i], d_r.at[ep], peer, tp)

    def dispatch_order(n):
        off = (n + 1) // 2
        return EP // 2 + off * (1 - 2 * (n % 2))

    def dispatch_all(n, carry):
        dispatch(dispatch_order(n)).start()
        return carry

    lax.fori_loop(0, EP - 1, dispatch_all, 0)

    def plus(d):
        block = 2 * (z - d) + core
        return remote(kv.at[block], kv.at[block], plus_s.at[d], plus_r.at[d + 1], ep + 2, tp)

    def plus_in(d):
        block = 2 * (z - d) + core
        return remote(kv.at[block], kv.at[block], plus_s.at[d - 1], plus_r.at[d], ep + 2, tp)

    def minus(d):
        block = 2 * ((z + d) % CHIPS) + core
        return remote(kv.at[block], kv.at[block], minus_s.at[d], minus_r.at[d + 1], (ep + EP - 2) % EP, tp)

    def minus_in(d):
        block = 2 * ((z + d) % CHIPS) + core
        return remote(kv.at[block], kv.at[block], minus_s.at[d - 1], minus_r.at[d], (ep + EP - 2) % EP, tp)

    def sibling(origin):
        block = 2 * origin + core
        return remote(kv.at[block], kv.at[block], sib_s.at[origin], sib_r.at[origin], sib, tp)

    def sibling_in(origin):
        block = 2 * origin + 1 - core
        return remote(kv.at[block], kv.at[block], sib_s.at[origin], sib_r.at[origin], sib, tp)

    far = 6

    def ring_open():
        @pl.when(z < CHIPS - 1)
        def _():
            plus(0).start()

        @pl.when(z <= far)
        def _():
            minus(0).start()

        @pl.when(core == 0)
        def _():
            sibling(z).start()

    def ring_step(d):
        @pl.when(z - d >= 0)
        def _():
            plus_in(d).wait_recv()
            if d < 8:
                @pl.when(z < CHIPS - 1)
                def _():
                    plus(d).start()
            sibling(z - d).start()

        if d <= 7:
            origin = (z + d) % CHIPS

            @pl.when(origin <= far)
            def _():
                minus_in(d).wait_recv()
                if d < 7:
                    minus(d).start()

                @pl.when(origin < z)
                def _():
                    sibling(origin).start()

    ring_open()

    xrec[ep] = xsend[ep]

    def dispatch_wait(i, carry):
        source = (ep + i) % EP
        remote(xsend.at[source], xrec.at[source], d_s.at[i], d_r.at[source], source, tp).wait_recv()
        return carry

    lax.fori_loop(1, EP, dispatch_wait, 0)
    pack = pack_ref[...]
    for h in range(2):
        got = jnp.concatenate([xrec[h * (EP // 2) + s] for s in range(EP // 2)], axis=0)
        xall[h * HALF : (h + 1) * HALF, lanes(tp)] = mm(pack, got).astype(BF16)

    top, low = pl.ds(0, HALF), pl.ds(HALF, HALF)

    def ag1(h, j):
        part = xall.at[(top, low)[h], lanes(tp)]
        return remote(part, part, ag1_s.at[h, j], ag1_r.at[h, j], ep, x_peer(j) if h == 0 else y_peer(j))

    def ag1_in(h, j):
        other = x_peer(SIDE - j) if h == 0 else y_peer(SIDE - j)
        part = xall.at[(top, low)[h], lanes(other)]
        return remote(part, part, ag1_s.at[h, j], ag1_r.at[h, j], ep, other)

    for j in (2, 1, 3):
        for h in range(2):
            ag1(h, j).start()
    ring_step(1)

    def ag2a(j, row):
        part = xall.at[top, lanes(row, BAND)]
        return remote(part, part, ag2_s.at[0, j], ag2_r.at[0, j], ep, y_peer(j))

    def ag2b(j, n, column):
        part = xall.at[low, lanes(n * SIDE + column)]
        return remote(part, part, ag2_s.at[1 + n, j], ag2_r.at[1 + n, j], ep, x_peer(j))

    for j in (1, 3, 2):
        ag1_in(0, j).wait_recv()
    for j in (2, 1, 3):
        ag2a(j, y).start()
    for j in (1, 3, 2):
        ag1_in(1, j).wait_recv()
    for j in (2, 1, 3):
        for n in range(SIDE):
            ag2b(j, n, x).start()
    ring_step(2)
    ring_step(3)
    ring_step(4)
    ring_step(5)

    for copy in weight_copies:
        copy.wait()

    def ffn(i, carry):
        rows = pl.ds(pl.multiple_of(i * TILE, TILE), TILE)
        block = xall[rows, :]
        gated = jnp.minimum(mm(block, gate_ref[...]), CLAMP_LIMIT)
        clipped = jnp.clip(mm(block, up_ref[...]), -CLAMP_LIMIT, CLAMP_LIMIT)
        active = ((clipped + 1.0) * gated * jax.nn.sigmoid(GATE_SLOPE * gated)).astype(BF16)
        ypart[rows, :] = mm(active, down_ref[...]).astype(BF16)
        return carry

    def rs1_a(j):
        to = (y + j) % SIDE
        return remote(ypart.at[top, lanes(to, BAND)], rs1a.at[j - 1], r1_s.at[0, j], r1_r.at[0, j], ep, y_peer(j))

    def rs1_b(j, n):
        to = (x + j) % SIDE
        return remote(
            ypart.at[low, lanes(n * SIDE + to)], rs1b.at[j - 1, n], r1_s.at[1 + n, j], r1_r.at[1 + n, j], ep, x_peer(j)
        )

    for j in (1, 3, 2):
        ag2a(j, (y + SIDE - j) % SIDE).wait_recv()
    lax.fori_loop(0, HALF // TILE, ffn, 0)
    for j in (2, 1, 3):
        rs1_a(j).start()
    for j in (1, 3, 2):
        for n in range(SIDE):
            ag2b(j, n, (x + SIDE - j) % SIDE).wait_recv()
    lax.fori_loop(HALF // TILE, 2 * HALF // TILE, ffn, 0)
    for j in (2, 1, 3):
        for n in range(SIDE):
            rs1_b(j, n).start()

    ring_step(6)
    ring_step(7)
    ring_step(8)

    column = lax.broadcasted_iota(jnp.int32, (TOK, LANE), 1)
    row = lax.broadcasted_iota(jnp.int32, (TOK, LANE), 0)
    query = qkv_ref[0] * jnp.asarray(0.125, BF16)
    nothing = jnp.zeros_like(query)
    queries = jnp.concatenate([jnp.where(column < 64, query, nothing), jnp.where(column < 64, nothing, query)], axis=0)
    causal = jnp.concatenate([column <= row, column <= row], axis=0)

    scores = jnp.where(causal, mm(queries, kv[ep, 0], NT), -jnp.inf)
    top_score = jnp.max(scores, axis=-1, keepdims=True)
    terms = jnp.exp(scores - top_score)
    m_ref[...] = jnp.broadcast_to(top_score, (2 * TOK, LANE))
    l_ref[...] = jnp.broadcast_to(jnp.sum(terms, axis=-1, keepdims=True), (2 * TOK, LANE))
    acc_ref[...] = mm(terms.astype(BF16), kv[ep, 1])

    def attend(keys, values):
        scores = mm(queries, keys, NT)
        old = m_ref[:, 0:1]
        new = jnp.maximum(old, jnp.max(scores, axis=-1, keepdims=True))
        shrink = jnp.exp(old - new)
        terms = jnp.exp(scores - new)
        m_ref[...] = jnp.broadcast_to(new, (2 * TOK, LANE))
        l_ref[...] = l_ref[...] * shrink + jnp.sum(terms, axis=-1, keepdims=True)
        acc_ref[...] = acc_ref[...] * shrink + mm(terms.astype(BF16), values)

    @pl.when(core == 1)
    def _():
        sibling_in(z).wait_recv()
        attend(kv[2 * z, 0], kv[2 * z, 1])

    def attend_chip(origin, carry):
        sibling_in(origin).wait_recv()
        keys = jnp.concatenate([kv[2 * origin, 0], kv[2 * origin + 1, 0]], axis=0)
        values = jnp.concatenate([kv[2 * origin, 1], kv[2 * origin + 1, 1]], axis=0)
        attend(keys, values)
        return carry

    lax.fori_loop(0, z, attend_chip, 0)
    ratio = acc_ref[...] / l_ref[...]
    attended = ratio[:TOK] - lam_ref[...] * ratio[TOK:]
    square = jnp.mean(attended * attended, axis=-1, keepdims=True)
    head = (attended * lax.rsqrt(square + NORM_EPS) * gain_ref[...]).astype(BF16)
    product = mm(head, ow_ref[...])
    for t in range(TP):
        psend[t] = product[t * 8 : (t + 1) * 8].astype(BF16)

    def share(i):
        peer = (tp + i) % TP
        return remote(psend.at[peer], prec.at[tp], p_s.at[i], p_r.at[tp], ep, peer)

    def share_start(i, carry):
        share(i).start()
        return carry

    lax.fori_loop(1, TP, share_start, 0)
    prec[tp] = psend[tp]

    def rs2_a(j):
        to = (x + j) % SIDE
        return remote(z0.at[:, lanes(to)], rs2a.at[j - 1], r2_s.at[0, j], r2_r.at[0, j], ep, x_peer(j))

    def rs2_b(j):
        to = (y + j) % SIDE
        return remote(z1.at[to], rs2b.at[j - 1], r2_s.at[1, j], r2_r.at[1, j], ep, y_peer(j))

    for j in (1, 3, 2):
        rs1_a(j).wait_recv()
    total = ypart[top, lanes(y, BAND)].astype(F32)
    for j in (1, 2, 3):
        total = total + rs1a[j - 1].astype(F32)
    z0[...] = total.astype(BF16)
    for j in (2, 1, 3):
        rs2_a(j).start()
    for j in (1, 3, 2):
        for n in range(SIDE):
            rs1_b(j, n).wait_recv()
    for n in range(SIDE):
        total = ypart[low, lanes(n * SIDE + x)].astype(F32)
        for j in (1, 2, 3):
            total = total + rs1b[j - 1, n].astype(F32)
        z1[n] = total.astype(BF16)
    for j in (2, 1, 3):
        rs2_b(j).start()

    unpack = unpack_ref[...]
    for j in (1, 3, 2):
        rs2_a(j).wait_recv()
    total = z0[:, lanes(x)].astype(F32)
    for j in (1, 2, 3):
        total = total + rs2a[j - 1].astype(F32)
    result = mm(unpack, total.astype(BF16)).astype(BF16)
    for s in range(EP // 2):
        rsend[s] = result[s * SLAB : (s + 1) * SLAB]
    for j in (1, 3, 2):
        rs2_b(j).wait_recv()
    total = z1[y].astype(F32)
    for j in (1, 2, 3):
        total = total + rs2b[j - 1].astype(F32)
    result = mm(unpack, total.astype(BF16)).astype(BF16)
    for s in range(EP // 2):
        rsend[EP // 2 + s] = result[s * SLAB : (s + 1) * SLAB]

    def give_back(i):
        peer = (ep + i) % EP
        return remote(rsend.at[peer], rrec.at[ep], b_s.at[i], b_r.at[ep], peer, tp)

    def give_back_start(n, carry):
        give_back(dispatch_order(n)).start()
        return carry

    lax.fori_loop(0, EP - 1, give_back_start, 0)
    rrec[ep] = rsend[ep]

    def share_wait(i, carry):
        source = (tp + i) % TP
        remote(psend.at[source], prec.at[source], p_s.at[i], p_r.at[source], ep, source).wait_recv()
        return carry

    lax.fori_loop(1, TP, share_wait, 0)
    total = prec[0].astype(F32)
    for t in range(1, TP):
        total = total + prec[t].astype(F32)
    rows_ref[...] = total.astype(BF16)

    slots = jnp.abs(mm(place.astype(BF16), spread, NT)) < 0.5
    parts = []
    rest = weight
    for _ in range(3):
        part = rest.astype(BF16)
        rest = rest - part.astype(F32)
        parts.append(jnp.where(slots, mm(part, spread, NT), 0.0).astype(BF16))

    def give_back_wait(i, carry):
        source = (ep + i) % EP
        remote(rsend.at[source], rrec.at[source], b_s.at[i], b_r.at[source], source, tp).wait_recv()
        return carry

    lax.fori_loop(1, EP, give_back_wait, 0)
    back = jnp.concatenate([rrec[e] for e in range(EP)], axis=0)
    combined = mm(parts[2], back) + mm(parts[1], back) + mm(parts[0], back)
    experts_ref[...] = combined.astype(BF16)

    def drain_ep(i, carry):
        dispatch(i).wait_send()
        give_back(i).wait_send()
        return carry

    lax.fori_loop(1, EP, drain_ep, 0)

    def drain_tp(i, carry):
        share(i).wait_send()
        return carry

    lax.fori_loop(1, TP, drain_tp, 0)
    for j in (1, 2, 3):
        for h in range(2):
            ag1(h, j).wait_send()
        ag2a(j, y).wait_send()
        rs1_a(j).wait_send()
        rs2_a(j).wait_send()
        rs2_b(j).wait_send()
        for n in range(SIDE):
            ag2b(j, n, x).wait_send()
            rs1_b(j, n).wait_send()
    for d in range(8):
        @pl.when((z < CHIPS - 1) & (z - d >= 0))
        def _():
            plus(d).wait_send()
    for d in range(7):
        @pl.when((z + d) % CHIPS <= far)
        def _():
            minus(d).wait_send()

    def drain_sibling(origin, carry):
        sibling(origin).wait_send()
        return carry

    lax.fori_loop(0, z + (1 - core), drain_sibling, 0)


def body(
    query_maps, key_maps, value_rows, head_lambda, head_gain, out_weight, token_rows, norm_gain, expert_ids,
    route_weights, gate_weight, up_weight, down_weight,
):
    qkv = jnp.stack([a.reshape(TOK, LANE) for a in (query_maps, key_maps, value_rows)])
    spread, pack, unpack = (jnp.asarray(a, BF16) for a in slot_tables())
    vmem = pl.BlockSpec(memory_space=pltpu.VMEM)
    hbm = pl.BlockSpec(memory_space=pl.ANY)
    dma = pltpu.SemaphoreType.DMA
    return pl.pallas_call(
        kernel,
        name="layer",
        out_shape=(jax.ShapeDtypeStruct((TOK // TP, D), BF16), jax.ShapeDtypeStruct((TOK, LANE), BF16)),
        in_specs=[vmem, vmem, vmem, hbm] + [vmem] * 7 + [hbm] * 3,
        out_specs=(vmem, vmem),
        scratch_shapes=[
            pltpu.VMEM((EP, 2, TOK, LANE), BF16),
            pltpu.VMEM((2 * TOK, LANE), F32),
            pltpu.VMEM((2 * TOK, LANE), F32),
            pltpu.VMEM((2 * TOK, LANE), F32),
            pltpu.VMEM((TP, TOK // TP, D), BF16),
            pltpu.VMEM((TP, TOK // TP, D), BF16),
            pltpu.VMEM((EP, SLAB, LANE), BF16),
            pltpu.VMEM((EP, SLAB, LANE), BF16),
            pltpu.VMEM((ROWS, D), BF16),
            pltpu.VMEM((ROWS, D), BF16),
            pltpu.VMEM((SIDE - 1, HALF, BAND), BF16),
            pltpu.VMEM((SIDE - 1, SIDE, HALF, LANE), BF16),
            pltpu.VMEM((HALF, BAND), BF16),
            pltpu.VMEM((SIDE, HALF, LANE), BF16),
            pltpu.VMEM((SIDE - 1, HALF, LANE), BF16),
            pltpu.VMEM((SIDE - 1, HALF, LANE), BF16),
            pltpu.VMEM((EP, SLAB, LANE), BF16),
            pltpu.VMEM((EP, SLAB, LANE), BF16),
            pltpu.VMEM((LANE, D), BF16),
            pltpu.VMEM((D, UNITS), BF16),
            pltpu.VMEM((D, UNITS), BF16),
            pltpu.VMEM((UNITS, D), BF16),
            dma((4,)),
            dma((8,)), dma((9,)), dma((7,)), dma((8,)), dma((CHIPS,)), dma((CHIPS,)),
            dma((TP,)), dma((TP,)), dma((EP,)), dma((EP,)),
            dma((2, SIDE)), dma((2, SIDE)), dma((1 + SIDE, SIDE)), dma((1 + SIDE, SIDE)),
            dma((1 + SIDE, SIDE)), dma((1 + SIDE, SIDE)), dma((2, SIDE)), dma((2, SIDE)),
            dma((EP,)), dma((EP,)),
        ],
        compiler_params=pltpu.CompilerParams(
            collective_id=0, has_side_effects=True, vmem_limit_bytes=60 * 1024 * 1024
        ),
    )(
        qkv, head_lambda.reshape(1, 1), head_gain.reshape(1, LANE), out_weight, token_rows,
        norm_gain.reshape(1, D), expert_ids, route_weights, spread, pack, unpack,
        gate_weight.reshape(D, UNITS), up_weight.reshape(D, UNITS), down_weight.reshape(UNITS, D),
    )


def solution(mesh):
    placed = (
        P("ep", "tp", None), P("ep", "tp", None), P("ep", "tp", None), P("tp"), P(), P("tp", None), P("ep", None),
        P(), P("ep", None), P("ep", None), P("ep", None, "tp"), P("ep", None, "tp"), P("ep", "tp", None),
    )
    return jax.shard_map(
        body, mesh=mesh, in_specs=placed, out_specs=(P(("ep", "tp"), None), P("ep", "tp")), check_vma=False
    )
```

```python
import functools

import jax
import jax.numpy as jnp
import numpy as np
from jax import lax
from jax.experimental import pallas as pl
from jax.experimental.pallas import tpu as pltpu
from jax.sharding import PartitionSpec as P

NORM_EPS = 1e-05
CLAMP_LIMIT = 7.0
GATE_SLOPE = 1.702
MESH = pl.DeviceIdType.MESH

EP, TP, SIDE, CHIPS = 32, 16, 4, 16
CAP, SLAB = 20, 24
CHUNKS = ((0, 1, 15, 2), (12, 5, 11, 6), (10, 7, 9, 8), (14, 3, 13, 4))
STEPS = len(CHUNKS)
SOURCES = EP // STEPS
ROWS = EP * CAP
TILE, PADDED_TILE = SOURCES * CAP, SOURCES * SLAB
HALF = TILE // 2
PADDED = EP * SLAB
D, LANE, TOK, UNITS = 2048, 128, 128, 256
BAND = SIDE * LANE
PAIR = 2 * LANE
FAR = 6
F32, BF16 = jnp.float32, jnp.bfloat16
NN = (((1,), (0,)), ((), ()))
NT = (((1,), (1,)), ((), ()))


def mm(a, b, dims=NN):
    return lax.dot_general(a, b, dims, preferred_element_type=F32)


def slot_tables():
    rows = np.arange(PADDED)
    spread = np.zeros((PADDED, LANE), np.float32)
    spread[rows, rows // SLAB] = 1.0
    spread[rows, EP] = -(rows % SLAB)
    pack = np.zeros((TILE, PADDED_TILE), np.float32)
    r = np.arange(TILE)
    pack[r, r // CAP * SLAB + r % CAP] = 1.0
    return spread, pack, pack.T.copy()


def kernel(
    q_hbm, k_hbm, v_hbm, lam_hbm, gain_hbm, ow_hbm, tok_hbm, ngain_hbm, ids_hbm, wts_hbm, spread_hbm, pack_hbm,
    unpack_hbm, gate_hbm, up_hbm, down_hbm,
    rows_ref, experts_ref,
    q_ref, lam_ref, gain_ref, ow_ref, tok_ref, ngain_ref, ids_ref, wts_ref, spread_ref, pack_ref, unpack_ref,
    gate_ref, up_ref, down_ref,
    kv, m_ref, l_ref, acc_ref, ps, pa, pb, pc, xsend, xrec, xall, ypart, rs1, comb, band, rs2, rsend, rrec,
    local_sem, plus_s, plus_r, minus_s, minus_r, sib_s, sib_r, sent, p_r, d_r, ag1_r, ag2_r, ag2_rest, r1_r, r1_rest,
    r2_r, b_r,
):
    ep = lax.axis_index("ep")
    tp = lax.axis_index("tp")
    z, core = ep // 2, ep % 2
    x, y = tp % SIDE, tp // SIDE
    sib = z * 2 + (1 - core)

    def lanes(block, width=LANE):
        return pl.ds(pl.multiple_of(block * width, width), width)

    def remote(src, dst, ssem, rsem, e, t):
        return pltpu.make_async_remote_copy(
            src_ref=src, dst_ref=dst, send_sem=ssem, recv_sem=rsem, device_id=(e, t), device_id_type=MESH
        )

    def arrived(ref, sem):
        remote(ref, ref, sent.at[0], sem, sib, tp).wait_recv()

    def left(ref, kind):
        remote(ref, ref, sent.at[kind], b_r.at[0], sib, tp).wait_send()

    def x_peer(j):
        return y * SIDE + (x + j) % SIDE

    def y_peer(j):
        return ((y + j) % SIDE) * SIDE + x

    barrier = pltpu.get_barrier_semaphore()

    def greet_ep(n, carry):
        off = (n + 1) // 2
        to = (ep + EP // 2 + off * (1 - 2 * (n % 2))) % EP
        pl.semaphore_signal(barrier, inc=1, device_id=(to, tp), device_id_type=MESH)
        return carry

    def greet_tp(i, carry):
        pl.semaphore_signal(barrier, inc=1, device_id=(ep, (tp + i) % TP), device_id_type=MESH)
        return carry

    lax.fori_loop(0, EP - 1, greet_ep, 0)
    lax.fori_loop(1, TP, greet_tp, 0)

    moves = (
        (tok_hbm, tok_ref), (ids_hbm, ids_ref), (wts_hbm, wts_ref), (ngain_hbm, ngain_ref), (spread_hbm, spread_ref),
        (q_hbm, q_ref), (k_hbm, kv.at[ep, 0]), (v_hbm, kv.at[ep, 1]), (pack_hbm, pack_ref), (unpack_hbm, unpack_ref),
        (lam_hbm, lam_ref), (gain_hbm, gain_ref),
        (gate_hbm, gate_ref), (up_hbm, up_ref), (down_hbm, down_ref), (ow_hbm, ow_ref),
    )
    local = [pltpu.make_async_copy(src, dst, local_sem.at[i]) for i, (src, dst) in enumerate(moves)]
    for copy in local:
        copy.start()
    for copy in local[:5]:
        copy.wait()

    tokens = tok_ref[...].astype(F32)
    scale = lax.rsqrt(jnp.mean(tokens * tokens, axis=-1, keepdims=True) + NORM_EPS)
    mine = tok_ref[:, lanes(tp)].astype(F32)
    normed = (mine * scale * ngain_ref[:, lanes(tp)]).astype(BF16)
    first = lax.broadcasted_iota(jnp.int32, (TOK, LANE), 0)
    second = lax.broadcasted_iota(jnp.int32, (TOK, LANE), 1)
    named = jnp.zeros((TOK, LANE), F32)
    weight = jnp.zeros((TOK, LANE), F32)
    for k in range(4):
        hit = ids_ref[k : k + 1, :] == first
        named = named + jnp.where(hit, 1.0, 0.0)
        weight = weight + jnp.where(hit, wts_ref[k : k + 1, :], 0.0)
    before = jnp.where(first < second, 1.0, 0.0).astype(BF16)
    rank = mm(named.astype(BF16), before)
    place = jnp.where(named > 0.5, rank, -1.0)
    place = jnp.where(first < EP, place, jnp.where(first == EP, 1.0, 0.0))
    chosen = mm(spread_ref[...], place.astype(BF16))
    chosen = jnp.where(jnp.abs(chosen) < 0.5, 1.0, 0.0).astype(BF16)
    outgoing = mm(chosen, normed).astype(BF16)
    for e in range(EP):
        xsend[e] = outgoing[e * SLAB : (e + 1) * SLAB]
    for copy in local[5:8]:
        copy.wait()

    pl.semaphore_wait(barrier, EP - 1 + TP - 1)

    members = [[(n, chip, c) for n, chip in enumerate(CHUNKS[k]) for c in range(2)] for k in range(STEPS)]

    def elsewhere(chip, c, do):
        if chip == 0:
            pl.when(core != c)(do)
        else:
            do()

    def dispatch(k, n, chip, c):
        to = 2 * ((z + chip) % CHIPS) + c
        slot = (k * len(CHUNKS[0]) + n) * 2
        return remote(xsend.at[to], xrec.at[slot + core], sent.at[0], d_r.at[k], to, tp)

    for k in range(STEPS):
        for n, chip, c in members[k]:
            elsewhere(chip, c, lambda: dispatch(k, n, chip, c).start())
    xrec[core] = xsend[ep]

    def plus(d):
        block = 2 * (z - d) + core
        return remote(kv.at[block], kv.at[block], plus_s.at[d], plus_r.at[d + 1], (ep + 2) % EP, tp)

    def plus_in(d):
        block = 2 * (z - d) + core
        return remote(kv.at[block], kv.at[block], plus_s.at[d - 1], plus_r.at[d], (ep + 2) % EP, tp)

    def minus(d):
        block = 2 * ((z + d) % CHIPS) + core
        return remote(kv.at[block], kv.at[block], minus_s.at[d], minus_r.at[d + 1], (ep + EP - 2) % EP, tp)

    def minus_in(d):
        block = 2 * ((z + d) % CHIPS) + core
        return remote(kv.at[block], kv.at[block], minus_s.at[d - 1], minus_r.at[d], (ep + EP - 2) % EP, tp)

    def sibling(origin):
        block = 2 * origin + core
        return remote(kv.at[block], kv.at[block], sib_s.at[origin], sib_r.at[origin], sib, tp)

    def sibling_in(origin):
        block = 2 * origin + 1 - core
        return remote(kv.at[block], kv.at[block], sib_s.at[origin], sib_r.at[origin], sib, tp)

    def ring_open():
        @pl.when(z < CHIPS - 1)
        def _():
            plus(0).start()

        @pl.when(z <= FAR)
        def _():
            minus(0).start()

        @pl.when(core == 0)
        def _():
            sibling(z).start()

    def ring_step(d):
        @pl.when(z - d >= 0)
        def _():
            plus_in(d).wait_recv()
            if d < 8:
                @pl.when(z < CHIPS - 1)
                def _():
                    plus(d).start()
            sibling(z - d).start()

        if d <= 7:
            origin = (z + d) % CHIPS

            @pl.when(origin <= FAR)
            def _():
                minus_in(d).wait_recv()
                if d < 7:
                    minus(d).start()

                @pl.when(origin < z)
                def _():
                    sibling(origin).start()

    far_first = (2, 1, 3)

    queries_of = []

    def attend(blocks):
        keys = jnp.concatenate([kv[b, 0] for b in blocks], axis=0)
        values = jnp.concatenate([kv[b, 1] for b in blocks], axis=0)
        scores = mm(queries_of[0], keys, NT)
        old = m_ref[:, 0:1]
        new = jnp.maximum(old, jnp.max(scores, axis=-1, keepdims=True))
        shrink = jnp.exp(old - new)
        terms = jnp.exp(scores - new)
        m_ref[...] = jnp.broadcast_to(new, (2 * TOK, LANE))
        l_ref[...] = l_ref[...] * shrink + jnp.sum(terms, axis=-1, keepdims=True)
        acc_ref[...] = acc_ref[...] * shrink + mm(terms.astype(BF16), values)

    def attend_open():
        query = q_ref[...] * jnp.asarray(0.125, BF16)
        nothing = jnp.zeros_like(query)
        queries = jnp.concatenate([jnp.where(second < 64, query, nothing), jnp.where(second < 64, nothing, query)], axis=0)
        queries_of.append(queries)
        causal = jnp.concatenate([second <= first, second <= first], axis=0)
        scores = jnp.where(causal, mm(queries, kv[ep, 0], NT), -jnp.inf)
        top_score = jnp.max(scores, axis=-1, keepdims=True)
        terms = jnp.exp(scores - top_score)
        m_ref[...] = jnp.broadcast_to(top_score, (2 * TOK, LANE))
        l_ref[...] = jnp.broadcast_to(jnp.sum(terms, axis=-1, keepdims=True), (2 * TOK, LANE))
        acc_ref[...] = mm(terms.astype(BF16), kv[ep, 1])

    def attend_pair():
        @pl.when(core == 1)
        def _():
            sibling_in(z).wait_recv()
            attend([2 * z])

    def attend_some(a, a_in, b, b_in):
        def both():
            sibling_in(a).wait_recv()
            sibling_in(b).wait_recv()
            attend([2 * a, 2 * a + 1, 2 * b, 2 * b + 1])

        def one():
            sibling_in(a).wait_recv()
            attend([2 * a, 2 * a + 1])

        pl.when(a_in & b_in)(both)
        pl.when(a_in & jnp.logical_not(b_in))(one)

    def attend_plus(d):
        attend_some(z - d, z - d >= 0, z - d - 1, z - d - 1 >= 0)

    def attend_minus(d):
        late, early = (z + d + 1) % CHIPS, (z + d) % CHIPS
        attend_some(late, z + d + 1 >= CHIPS, early, z + d >= CHIPS)

    def attend_last():
        origin = (z + 7) % CHIPS

        @pl.when(z + 7 >= CHIPS)
        def _():
            sibling_in(origin).wait_recv()
            attend([2 * origin, 2 * origin + 1])

    def attend_close():
        ratio = acc_ref[...] / l_ref[...]
        attended = ratio[:TOK] - lam_ref[...] * ratio[TOK:]
        square = jnp.mean(attended * attended, axis=-1, keepdims=True)
        head = (attended * lax.rsqrt(square + NORM_EPS) * gain_ref[...]).astype(BF16)
        product = mm(head, ow_ref[...])
        for q in range(SIDE):
            ps[0, q] = product[q * 32 : (q + 1) * 32, : D // 2].astype(BF16)
            picked = [product[(n * SIDE + q) * 8 : (n * SIDE + q) * 8 + 8, D // 2 :] for n in range(SIDE)]
            ps[1, q] = jnp.concatenate(picked, axis=0).astype(BF16)
        for j in far_first:
            for h in range(2):
                share_first(h, j).start()

    def share_first(h, j):
        to = (second_at[h] + j) % SIDE
        return remote(ps.at[h, to], pa.at[h, j - 1], sent.at[6], p_r.at[0], ep, along(h, j))

    def share_second(h, j):
        to = (first_at[h] + j) % SIDE
        return remote(pb.at[h, to], pc.at[h, j - 1], sent.at[7], p_r.at[1], ep, across(h, j))

    def share_sum():
        arrived(pa, p_r.at[0])
        for h in range(2):
            total = ps[h, second_at[h]].astype(F32)
            for j in (1, 2, 3):
                total = total + pa[h, j - 1].astype(F32)
            for n in range(SIDE):
                pb[h, n] = total[n * 8 : (n + 1) * 8].astype(BF16)
            for j in far_first:
                share_second(h, j).start()

    def rows(k, h):
        return pl.ds(k * TILE + h * HALF, HALF)

    def ag1(k, h, j):
        part = xall.at[rows(k, h), lanes(tp)]
        return remote(part, part, sent.at[1], ag1_r.at[k], ep, x_peer(j) if h == 0 else y_peer(j))

    second_at = (y, x)
    first_at = (x, y)

    def along(h, j):
        return y_peer(j) if h == 0 else x_peer(j)

    def across(h, j):
        return x_peer(j) if h == 0 else y_peer(j)

    def columns(h, q, half):
        q = q % SIDE
        if h == 0:
            return [lanes(2 * q + half, PAIR)]
        return [lanes((2 * half + i) * SIDE + q) for i in range(2)]

    def pieces(h):
        return range(1 + h)

    def ahead(s):
        return 1 if s == 0 else SIDE - 1

    def behind(s):
        return SIDE - ahead(s)

    def ag2(k, h, s, half, i, q):
        part = xall.at[rows(k, h), columns(h, q, half)[i]]
        sem = ag2_r.at[k, h, s] if half == s else ag2_rest.at[k]
        return remote(part, part, sent.at[2], sem, ep, along(h, ahead(s)))

    def ag2_relay(k, h, s, i, q):
        part = xall.at[rows(k, h), columns(h, q, s)[i]]
        return remote(part, part, sent.at[2], ag2_rest.at[k], ep, along(h, ahead(s)))

    def rs1_raw(k, h, s, kind, i):
        q, half = (second_at[h] + 2, s) if kind == 0 else (second_at[h] + ahead(s), 1 - s)
        part = ypart.at[rows(k, h), columns(h, q, half)[i]]
        to = rs1.at[k, h, kind, s] if h == 0 else rs1.at[k, h, kind, s, :, pl.ds(i * LANE, LANE)]
        sem = r1_r.at[k, h, s] if kind == 0 else r1_rest.at[k, h]
        return remote(part, to, sent.at[3], sem, ep, along(h, ahead(s)))

    def rs1_comb(k, h, s):
        return remote(comb.at[k, h, s], rs1.at[k, h, 2, s], sent.at[3], r1_rest.at[k, h], ep, along(h, ahead(s)))

    def share_of(k, h, q, half):
        return jnp.concatenate([ypart[rows(k, h), c].astype(F32) for c in columns(h, q, half)], axis=1)

    def rs2_copy(k, h, j):
        part = band.at[k, h, :, lanes((first_at[h] + j) % SIDE)]
        return remote(part, rs2.at[k, h, j - 1], sent.at[4], r2_r.at[k], ep, across(h, j))

    def give_back(k, n, chip, c):
        to = 2 * ((z + CHIPS - chip) % CHIPS) + c
        slot = (k * len(CHUNKS[0]) + n) * 2 + c
        return remote(rsend.at[slot], rrec.at[ep], sent.at[5], b_r.at[0], to, tp)


    def gather_open(k):
        arrived(xrec.at[pl.ds(k * SOURCES, SOURCES - (k == 0))], d_r.at[k])
        got = jnp.concatenate([xrec[k * SOURCES + s] for s in range(SOURCES)], axis=0)
        xall[k * TILE : (k + 1) * TILE, lanes(tp)] = mm(pack_ref[...], got).astype(BF16)
        for j in far_first:
            for h in range(2):
                ag1(k, h, j).start()

    def gather_more(k):
        arrived(xall.at[pl.ds(k * TILE, TILE), pl.ds(0, (SIDE - 1) * LANE)], ag1_r.at[k])
        for turn in range(2):
            for h in range(2):
                for s in range(2):
                    for i in pieces(h):
                        ag2(k, h, s, (s + turn) % 2, i, second_at[h]).start()

    def gather_relay(k):
        for h in range(2):
            for s in range(2):
                arrived(xall.at[rows(k, h), pl.ds(0, PAIR)], ag2_r.at[k, h, s])
                for i in pieces(h):
                    ag2_relay(k, h, s, i, second_at[h] + behind(s)).start()

    def experts(k):
        arrived(xall.at[pl.ds(k * TILE, TILE), pl.ds(0, 4 * PAIR)], ag2_rest.at[k])
        block = xall[k * TILE : (k + 1) * TILE, :]
        gated = jnp.minimum(mm(block, gate_ref[...]), CLAMP_LIMIT)
        clipped = jnp.clip(mm(block, up_ref[...]), -CLAMP_LIMIT, CLAMP_LIMIT)
        active = ((clipped + 1.0) * gated * jax.nn.sigmoid(GATE_SLOPE * gated)).astype(BF16)
        ypart[k * TILE : (k + 1) * TILE, :] = mm(active, down_ref[...]).astype(BF16)
        for kind in range(2):
            for h in range(2):
                for s in range(2):
                    for i in pieces(h):
                        rs1_raw(k, h, s, kind, i).start()

    def sum_relay(k):
        for h in range(2):
            for s in range(2):
                arrived(rs1.at[k, h, 0, s], r1_r.at[k, h, s])
                own = share_of(k, h, second_at[h] + ahead(s), s)
                comb[k, h, s] = (own + rs1[k, h, 0, s].astype(F32)).astype(BF16)
                rs1_comb(k, h, s).start()

    def sum_open(k):
        for h in range(2):
            arrived(rs1.at[k, h, pl.ds(1, 2)], r1_rest.at[k, h])
            for half in range(2):
                own = share_of(k, h, second_at[h], half)
                total = own + rs1[k, h, 2, half].astype(F32) + rs1[k, h, 1, 1 - half].astype(F32)
                band[k, h, :, half * PAIR : (half + 1) * PAIR] = total.astype(BF16)
            for j in far_first:
                rs2_copy(k, h, j).start()

    def sum_close(k):
        halves = []
        arrived(rs2.at[k], r2_r.at[k])
        for h in range(2):
            total = band[k, h, :, lanes(first_at[h])].astype(F32)
            for j in (1, 2, 3):
                total = total + rs2[k, h, j - 1].astype(F32)
            halves.append(total)
        total = jnp.concatenate(halves, axis=0).astype(BF16)
        result = mm(unpack_ref[...], total).astype(BF16)
        for s in range(SOURCES):
            rsend[k * SOURCES + s] = result[s * SLAB : (s + 1) * SLAB]
        for n, chip, c in members[k]:
            elsewhere(chip, c, lambda: give_back(k, n, chip, c).start())
        if k == 0:
            rrec[ep] = rsend[core]

    for copy in local[8:]:
        copy.wait()
    attend_open()
    gather_open(0)
    ring_open()
    gather_more(0)
    gather_open(1)
    ring_step(1)
    gather_relay(0)
    gather_open(2)
    gather_open(3)
    gather_more(1)
    ring_step(2)
    gather_more(2)
    experts(0)
    gather_more(3)
    attend_pair()
    ring_step(3)
    gather_relay(1)
    gather_relay(2)
    sum_relay(0)
    ring_step(4)
    attend_plus(1)
    attend_minus(1)
    experts(1)
    gather_relay(3)
    ring_step(5)
    sum_open(0)
    sum_relay(1)
    experts(2)
    ring_step(6)
    attend_plus(3)
    attend_minus(3)
    sum_close(0)
    sum_open(1)
    sum_relay(2)
    experts(3)
    ring_step(7)
    sum_close(1)
    sum_open(2)
    attend_plus(5)
    attend_minus(5)
    sum_relay(3)
    ring_step(8)
    sum_close(2)
    sum_open(3)
    attend_plus(7)
    attend_last()
    attend_close()

    places = jnp.transpose(place).astype(BF16)
    slots = jnp.abs(mm(places, spread_ref[...], NT)) < 0.5
    parts = []
    rest = jnp.transpose(weight)
    for _ in range(3):
        part = rest.astype(BF16)
        rest = rest - part.astype(F32)
        parts.append(jnp.where(slots, mm(part, spread_ref[...], NT), 0.0).astype(BF16))

    sum_close(3)
    share_sum()

    left(xsend.at[pl.ds(0, EP - 1)], 0)
    left(xall.at[pl.ds(0, TILE), pl.ds(0, 12 * LANE)], 1)
    left(xall.at[:, pl.ds(0, 12 * LANE)], 2)
    left(ypart.at[:, pl.ds(0, 12 * LANE)], 3)
    left(ypart.at[pl.ds(0, TILE), pl.ds(0, 12 * LANE)], 4)
    left(pa, 6)
    left(pc, 7)

    for d in range(8):
        @pl.when((z < CHIPS - 1) & (z - d >= 0))
        def _():
            plus(d).wait_send()
    for d in range(7):
        @pl.when((z + d) % CHIPS <= FAR)
        def _():
            minus(d).wait_send()

    def drain_sibling(origin, carry):
        sibling(origin).wait_send()
        return carry

    lax.fori_loop(0, z + (1 - core), drain_sibling, 0)

    arrived(pc, p_r.at[1])
    for h in range(2):
        total = pb[h, first_at[h]].astype(F32)
        for j in (1, 2, 3):
            total = total + pc[h, j - 1].astype(F32)
        rows_ref[:, h * (D // 2) : (h + 1) * (D // 2)] = total.astype(BF16)

    arrived(rrec.at[pl.ds(0, EP - 1)], b_r.at[0])
    back = jnp.concatenate([rrec[e] for e in range(EP)], axis=0)
    combined = mm(parts[2], back) + mm(parts[1], back) + mm(parts[0], back)
    experts_ref[...] = combined.astype(BF16)
    left(rsend.at[pl.ds(0, EP - 1)], 5)


def body(
    query_maps, key_maps, value_rows, head_lambda, head_gain, out_weight, token_rows, norm_gain, expert_ids,
    route_weights, gate_weight, up_weight, down_weight,
):
    spread, pack, unpack = (jnp.asarray(a, BF16) for a in slot_tables())
    vmem = pl.BlockSpec(memory_space=pltpu.VMEM)
    hbm = pl.BlockSpec(memory_space=pl.ANY)
    dma = pltpu.SemaphoreType.DMA
    return pl.pallas_call(
        kernel,
        name="layer",
        out_shape=(jax.ShapeDtypeStruct((TOK // TP, D), BF16), jax.ShapeDtypeStruct((TOK, LANE), BF16)),
        in_specs=[hbm] * 16,
        out_specs=(vmem, vmem),
        scratch_shapes=[
            pltpu.VMEM((TOK, LANE), BF16),
            pltpu.VMEM((1, 1), F32),
            pltpu.VMEM((1, LANE), F32),
            pltpu.VMEM((LANE, D), BF16),
            pltpu.VMEM((TOK, D), BF16),
            pltpu.VMEM((1, D), F32),
            pltpu.VMEM((4, TOK), jnp.int32),
            pltpu.VMEM((4, TOK), F32),
            pltpu.VMEM((PADDED, LANE), BF16),
            pltpu.VMEM((TILE, PADDED_TILE), BF16),
            pltpu.VMEM((PADDED_TILE, TILE), BF16),
            pltpu.VMEM((D, UNITS), BF16),
            pltpu.VMEM((D, UNITS), BF16),
            pltpu.VMEM((UNITS, D), BF16),
            pltpu.VMEM((EP, 2, TOK, LANE), BF16),
            pltpu.VMEM((2 * TOK, LANE), F32),
            pltpu.VMEM((2 * TOK, LANE), F32),
            pltpu.VMEM((2 * TOK, LANE), F32),
            pltpu.VMEM((2, SIDE, 32, D // 2), BF16),
            pltpu.VMEM((2, SIDE - 1, 32, D // 2), BF16),
            pltpu.VMEM((2, SIDE, 8, D // 2), BF16),
            pltpu.VMEM((2, SIDE - 1, 8, D // 2), BF16),
            pltpu.VMEM((EP, SLAB, LANE), BF16),
            pltpu.VMEM((EP, SLAB, LANE), BF16),
            pltpu.VMEM((ROWS, D), BF16),
            pltpu.VMEM((ROWS, D), BF16),
            pltpu.VMEM((STEPS, 2, 3, 2, HALF, PAIR), BF16),
            pltpu.VMEM((STEPS, 2, 2, HALF, PAIR), BF16),
            pltpu.VMEM((STEPS, 2, HALF, BAND), BF16),
            pltpu.VMEM((STEPS, 2, SIDE - 1, HALF, LANE), BF16),
            pltpu.VMEM((EP, SLAB, LANE), BF16),
            pltpu.VMEM((EP, SLAB, LANE), BF16),
            dma((16,)),
            dma((8,)), dma((9,)), dma((7,)), dma((8,)), dma((CHIPS,)), dma((CHIPS,)),
            dma((8,)), dma((2,)), dma((STEPS,)), dma((STEPS,)), dma((STEPS, 2, 2)), dma((STEPS,)), dma((STEPS, 2, 2)),
            dma((STEPS, 2)), dma((STEPS,)), dma((1,)),
        ],
        compiler_params=pltpu.CompilerParams(
            collective_id=0, has_side_effects=True, vmem_limit_bytes=60 * 1024 * 1024
        ),
    )(
        query_maps.reshape(TOK, LANE), key_maps.reshape(TOK, LANE), value_rows.reshape(TOK, LANE),
        head_lambda.reshape(1, 1), head_gain.reshape(1, LANE), out_weight, token_rows, norm_gain.reshape(1, D),
        expert_ids.T, route_weights.T, spread, pack, unpack,
        gate_weight.reshape(D, UNITS), up_weight.reshape(D, UNITS), down_weight.reshape(UNITS, D),
    )


def solution(mesh):
    placed = (
        P("ep", "tp", None), P("ep", "tp", None), P("ep", "tp", None), P("tp"), P(), P("tp", None), P("ep", None),
        P(), P("ep", None), P("ep", None), P("ep", None, "tp"), P("ep", None, "tp"), P("ep", "tp", None),
    )
    return jax.shard_map(
        body, mesh=mesh, in_specs=placed, out_specs=(P(("ep", "tp"), None), P("ep", "tp")), check_vma=False
    )
```

```python
import functools

import jax
import jax.numpy as jnp
import numpy as np
from jax import lax
from jax.experimental import pallas as pl
from jax.experimental.pallas import tpu as pltpu
from jax.sharding import PartitionSpec as P

NORM_EPS = 1e-05
CLAMP_LIMIT = 7.0
GATE_SLOPE = 1.702
MESH = pl.DeviceIdType.MESH

EP, TP, SIDE, CHIPS = 32, 16, 4, 16
CAP, SLAB = 20, 24
ORDER = ((0, 1, 2, 3), (1, 0, 3, 2), (2, 0, 1, 3), (3, 0, 1, 2))
OUTWARD = ((0, 2, 1, 3), (1, 0, 2, 3), (2, 0, 1, 3), (3, 1, 0, 2))
STEPS = len(ORDER)
SOURCES = EP // STEPS
ROWS = EP * CAP
TILE, PADDED_TILE = SOURCES * CAP, SOURCES * SLAB
HALF = TILE // 2
PADDED = EP * SLAB
D, LANE, TOK, UNITS = 2048, 128, 128, 256
BAND = SIDE * LANE
PAIR = 2 * LANE
FAR = 6
F32, BF16 = jnp.float32, jnp.bfloat16
NN = (((1,), (0,)), ((), ()))
NT = (((1,), (1,)), ((), ()))


def mm(a, b, dims=NN):
    return lax.dot_general(a, b, dims, preferred_element_type=F32)


def slot_tables():
    rows = np.arange(PADDED)
    spread = np.zeros((PADDED, LANE), np.float32)
    spread[rows, rows // SLAB] = 1.0
    spread[rows, EP] = -(rows % SLAB)
    pack = np.zeros((TILE, PADDED_TILE), np.float32)
    r = np.arange(TILE)
    pack[r, r // CAP * SLAB + r % CAP] = 1.0
    return spread, pack, pack.T.copy()


def kernel(
    q_hbm, k_hbm, v_hbm, lam_hbm, gain_hbm, ow_hbm, tok_hbm, ngain_hbm, ids_hbm, wts_hbm, spread_hbm, pack_hbm,
    unpack_hbm, gate_hbm, up_hbm, down_hbm,
    rows_ref, experts_ref,
    q_ref, lam_ref, gain_ref, ow_ref, tok_ref, ngain_ref, ids_ref, wts_ref, spread_ref, pack_ref, unpack_ref,
    gate_ref, up_ref, down_ref,
    kv, m_ref, l_ref, acc_ref, ps, pa, pb, pc, xsend, xrec, xall, ypart, rs1, comb, band, rs2, rsend, rrec,
    local_sem, plus_s, plus_r, minus_s, minus_r, sib_s, sib_r, sent, p_r, d_r, ag1_r, ag2_r, ag2_rest, r1_r, r1_rest,
    r2_r, b_r,
):
    ep = lax.axis_index("ep")
    tp = lax.axis_index("tp")
    z, core = ep // 2, ep % 2
    x, y = tp % SIDE, tp // SIDE
    sib = z * 2 + (1 - core)

    def lanes(block, width=LANE):
        return pl.ds(pl.multiple_of(block * width, width), width)

    def remote(src, dst, ssem, rsem, e, t):
        return pltpu.make_async_remote_copy(
            src_ref=src, dst_ref=dst, send_sem=ssem, recv_sem=rsem, device_id=(e, t), device_id_type=MESH
        )

    def arrived(ref, sem):
        remote(ref, ref, sent.at[0], sem, sib, tp).wait_recv()

    def left(ref, kind):
        remote(ref, ref, sent.at[kind], b_r.at[0], sib, tp).wait_send()

    def x_peer(j):
        return y * SIDE + (x + j) % SIDE

    def y_peer(j):
        return ((y + j) % SIDE) * SIDE + x

    barrier = pltpu.get_barrier_semaphore()

    def greet_ep(n, carry):
        off = (n + 1) // 2
        to = (ep + EP // 2 + off * (1 - 2 * (n % 2))) % EP
        pl.semaphore_signal(barrier, inc=1, device_id=(to, tp), device_id_type=MESH)
        return carry

    def greet_tp(i, carry):
        pl.semaphore_signal(barrier, inc=1, device_id=(ep, (tp + i) % TP), device_id_type=MESH)
        return carry

    lax.fori_loop(0, EP - 1, greet_ep, 0)
    lax.fori_loop(1, TP, greet_tp, 0)

    moves = (
        (tok_hbm, tok_ref), (ids_hbm, ids_ref), (wts_hbm, wts_ref), (ngain_hbm, ngain_ref), (spread_hbm, spread_ref),
        (q_hbm, q_ref), (k_hbm, kv.at[ep, 0]), (v_hbm, kv.at[ep, 1]), (pack_hbm, pack_ref), (unpack_hbm, unpack_ref),
        (lam_hbm, lam_ref), (gain_hbm, gain_ref),
        (gate_hbm, gate_ref), (up_hbm, up_ref), (down_hbm, down_ref), (ow_hbm, ow_ref),
    )
    local = [pltpu.make_async_copy(src, dst, local_sem.at[i]) for i, (src, dst) in enumerate(moves)]
    for copy in local:
        copy.start()
    for copy in local[:5]:
        copy.wait()

    tokens = tok_ref[...].astype(F32)
    scale = lax.rsqrt(jnp.mean(tokens * tokens, axis=-1, keepdims=True) + NORM_EPS)
    mine = tok_ref[:, lanes(tp)].astype(F32)
    normed = (mine * scale * ngain_ref[:, lanes(tp)]).astype(BF16)
    first = lax.broadcasted_iota(jnp.int32, (TOK, LANE), 0)
    second = lax.broadcasted_iota(jnp.int32, (TOK, LANE), 1)
    named = jnp.zeros((TOK, LANE), F32)
    weight = jnp.zeros((TOK, LANE), F32)
    for k in range(4):
        hit = ids_ref[k : k + 1, :] == first
        named = named + jnp.where(hit, 1.0, 0.0)
        weight = weight + jnp.where(hit, wts_ref[k : k + 1, :], 0.0)
    before = jnp.where(first < second, 1.0, 0.0).astype(BF16)
    rank = mm(named.astype(BF16), before)
    place = jnp.where(named > 0.5, rank, -1.0)
    place = jnp.where(first < EP, place, jnp.where(first == EP, 1.0, 0.0))
    chosen = mm(spread_ref[...], place.astype(BF16))
    chosen = jnp.where(jnp.abs(chosen) < 0.5, 1.0, 0.0).astype(BF16)
    outgoing = mm(chosen, normed).astype(BF16)
    for e in range(EP):
        xsend[e] = outgoing[e * SLAB : (e + 1) * SLAB]
    for copy in local[5:8]:
        copy.wait()

    pl.semaphore_wait(barrier, EP - 1 + TP - 1)

    quarter = z // (CHIPS // STEPS)

    def pick(table, n):
        at = [row[n] for row in table]
        reached = [(quarter + STEPS - i) // STEPS for i in range(1, STEPS)]
        return at[0] + sum((at[i] - at[i - 1]) * reached[i - 1] for i in range(1, STEPS))

    chunk = [pick(ORDER, k) for k in range(STEPS)]
    outward = [pick(OUTWARD, n) for n in range(STEPS)]

    def others(n):
        return range(1 if n == 0 else 0, SOURCES)

    def dispatch(n, i):
        to = outward[n] * SOURCES + (ep + i) % SOURCES
        return remote(xsend.at[to], xrec.at[ep], sent.at[0], d_r.at[quarter], to, tp)

    for n in range(STEPS):
        for i in others(n):
            dispatch(n, i).start()
    xrec[ep] = xsend[ep]

    def plus(d):
        block = 2 * (z - d) + core
        return remote(kv.at[block], kv.at[block], plus_s.at[d], plus_r.at[d + 1], (ep + 2) % EP, tp)

    def plus_in(d):
        block = 2 * (z - d) + core
        return remote(kv.at[block], kv.at[block], plus_s.at[d - 1], plus_r.at[d], (ep + 2) % EP, tp)

    def minus(d):
        block = 2 * ((z + d) % CHIPS) + core
        return remote(kv.at[block], kv.at[block], minus_s.at[d], minus_r.at[d + 1], (ep + EP - 2) % EP, tp)

    def minus_in(d):
        block = 2 * ((z + d) % CHIPS) + core
        return remote(kv.at[block], kv.at[block], minus_s.at[d - 1], minus_r.at[d], (ep + EP - 2) % EP, tp)

    def sibling(origin):
        block = 2 * origin + core
        return remote(kv.at[block], kv.at[block], sib_s.at[origin], sib_r.at[origin], sib, tp)

    def sibling_in(origin):
        block = 2 * origin + 1 - core
        return remote(kv.at[block], kv.at[block], sib_s.at[origin], sib_r.at[origin], sib, tp)

    def ring_open():
        @pl.when(z < CHIPS - 1)
        def _():
            plus(0).start()

        @pl.when(z <= FAR)
        def _():
            minus(0).start()

        @pl.when(core == 0)
        def _():
            sibling(z).start()

    def ring_step(d):
        @pl.when(z - d >= 0)
        def _():
            plus_in(d).wait_recv()
            if d < 8:
                @pl.when(z < CHIPS - 1)
                def _():
                    plus(d).start()
            sibling(z - d).start()

        if d <= 7:
            origin = (z + d) % CHIPS

            @pl.when(origin <= FAR)
            def _():
                minus_in(d).wait_recv()
                if d < 7:
                    minus(d).start()

                @pl.when(origin < z)
                def _():
                    sibling(origin).start()

    far_first = (2, 1, 3)

    queries_of = []

    def attend(blocks):
        keys = jnp.concatenate([kv[b, 0] for b in blocks], axis=0)
        values = jnp.concatenate([kv[b, 1] for b in blocks], axis=0)
        scores = mm(queries_of[0], keys, NT)
        old = m_ref[:, 0:1]
        new = jnp.maximum(old, jnp.max(scores, axis=-1, keepdims=True))
        shrink = jnp.exp(old - new)
        terms = jnp.exp(scores - new)
        m_ref[...] = jnp.broadcast_to(new, (2 * TOK, LANE))
        l_ref[...] = l_ref[...] * shrink + jnp.sum(terms, axis=-1, keepdims=True)
        acc_ref[...] = acc_ref[...] * shrink + mm(terms.astype(BF16), values)

    def attend_open():
        query = q_ref[...] * jnp.asarray(0.125, BF16)
        nothing = jnp.zeros_like(query)
        queries = jnp.concatenate([jnp.where(second < 64, query, nothing), jnp.where(second < 64, nothing, query)], axis=0)
        queries_of.append(queries)
        causal = jnp.concatenate([second <= first, second <= first], axis=0)
        scores = jnp.where(causal, mm(queries, kv[ep, 0], NT), -jnp.inf)
        top_score = jnp.max(scores, axis=-1, keepdims=True)
        terms = jnp.exp(scores - top_score)
        m_ref[...] = jnp.broadcast_to(top_score, (2 * TOK, LANE))
        l_ref[...] = jnp.broadcast_to(jnp.sum(terms, axis=-1, keepdims=True), (2 * TOK, LANE))
        acc_ref[...] = mm(terms.astype(BF16), kv[ep, 1])

    def attend_pair():
        @pl.when(core == 1)
        def _():
            sibling_in(z).wait_recv()
            attend([2 * z])

    def attend_some(a, a_in, b, b_in):
        def both():
            sibling_in(a).wait_recv()
            sibling_in(b).wait_recv()
            attend([2 * a, 2 * a + 1, 2 * b, 2 * b + 1])

        def one():
            sibling_in(a).wait_recv()
            attend([2 * a, 2 * a + 1])

        pl.when(a_in & b_in)(both)
        pl.when(a_in & jnp.logical_not(b_in))(one)

    def attend_plus(d):
        attend_some(z - d, z - d >= 0, z - d - 1, z - d - 1 >= 0)

    def attend_minus(d):
        late, early = (z + d + 1) % CHIPS, (z + d) % CHIPS
        attend_some(late, z + d + 1 >= CHIPS, early, z + d >= CHIPS)

    def attend_last():
        origin = (z + 7) % CHIPS

        @pl.when(z + 7 >= CHIPS)
        def _():
            sibling_in(origin).wait_recv()
            attend([2 * origin, 2 * origin + 1])

    def attend_close():
        ratio = acc_ref[...] / l_ref[...]
        attended = ratio[:TOK] - lam_ref[...] * ratio[TOK:]
        square = jnp.mean(attended * attended, axis=-1, keepdims=True)
        head = (attended * lax.rsqrt(square + NORM_EPS) * gain_ref[...]).astype(BF16)
        product = mm(head, ow_ref[...])
        for q in range(SIDE):
            ps[0, q] = product[q * 32 : (q + 1) * 32, : D // 2].astype(BF16)
            picked = [product[(n * SIDE + q) * 8 : (n * SIDE + q) * 8 + 8, D // 2 :] for n in range(SIDE)]
            ps[1, q] = jnp.concatenate(picked, axis=0).astype(BF16)
        for j in far_first:
            for h in range(2):
                share_first(h, j).start()

    def share_first(h, j):
        to = (second_at[h] + j) % SIDE
        return remote(ps.at[h, to], pa.at[h, j - 1], sent.at[6], p_r.at[0], ep, along(h, j))

    def share_second(h, j):
        to = (first_at[h] + j) % SIDE
        return remote(pb.at[h, to], pc.at[h, j - 1], sent.at[7], p_r.at[1], ep, across(h, j))

    def share_sum():
        arrived(pa, p_r.at[0])
        for h in range(2):
            total = ps[h, second_at[h]].astype(F32)
            for j in (1, 2, 3):
                total = total + pa[h, j - 1].astype(F32)
            for n in range(SIDE):
                pb[h, n] = total[n * 8 : (n + 1) * 8].astype(BF16)
            for j in far_first:
                share_second(h, j).start()

    def rows(k, h):
        return pl.ds(pl.multiple_of(chunk[k] * TILE + h * HALF, HALF), HALF)

    def all_rows(k):
        return pl.ds(pl.multiple_of(chunk[k] * TILE, TILE), TILE)

    def ag1(k, h, j):
        part = xall.at[rows(k, h), lanes(tp)]
        return remote(part, part, sent.at[1], ag1_r.at[k], ep, x_peer(j) if h == 0 else y_peer(j))

    second_at = (y, x)
    first_at = (x, y)

    def along(h, j):
        return y_peer(j) if h == 0 else x_peer(j)

    def across(h, j):
        return x_peer(j) if h == 0 else y_peer(j)

    def columns(h, q, half):
        q = q % SIDE
        if h == 0:
            return [lanes(2 * q + half, PAIR)]
        return [lanes((2 * half + i) * SIDE + q) for i in range(2)]

    def pieces(h):
        return range(1 + h)

    def ahead(s):
        return 1 if s == 0 else SIDE - 1

    def behind(s):
        return SIDE - ahead(s)

    def ag2(k, h, s, half, i, q):
        part = xall.at[rows(k, h), columns(h, q, half)[i]]
        sem = ag2_r.at[k, h, s] if half == s else ag2_rest.at[k]
        return remote(part, part, sent.at[2], sem, ep, along(h, ahead(s)))

    def ag2_relay(k, h, s, i, q):
        part = xall.at[rows(k, h), columns(h, q, s)[i]]
        return remote(part, part, sent.at[2], ag2_rest.at[k], ep, along(h, ahead(s)))

    def rs1_raw(k, h, s, kind, i):
        q, half = (second_at[h] + 2, s) if kind == 0 else (second_at[h] + ahead(s), 1 - s)
        part = ypart.at[rows(k, h), columns(h, q, half)[i]]
        to = rs1.at[k, h, kind, s] if h == 0 else rs1.at[k, h, kind, s, :, pl.ds(i * LANE, LANE)]
        sem = r1_r.at[k, h, s] if kind == 0 else r1_rest.at[k, h]
        return remote(part, to, sent.at[3], sem, ep, along(h, ahead(s)))

    def rs1_comb(k, h, s):
        return remote(comb.at[k, h, s], rs1.at[k, h, 2, s], sent.at[3], r1_rest.at[k, h], ep, along(h, ahead(s)))

    def share_of(k, h, q, half):
        return jnp.concatenate([ypart[rows(k, h), c].astype(F32) for c in columns(h, q, half)], axis=1)

    def rs2_copy(k, h, j):
        part = band.at[k, h, :, lanes((first_at[h] + j) % SIDE)]
        return remote(part, rs2.at[k, h, j - 1], sent.at[4], r2_r.at[k], ep, across(h, j))

    def give_back(k, i):
        to = chunk[k] * SOURCES + (ep + i) % SOURCES
        return remote(rsend.at[to], rrec.at[ep], sent.at[5], b_r.at[0], to, tp)

    def gather_open(k):
        arrived(xrec.at[pl.ds(chunk[k] * SOURCES, len(others(k)))], d_r.at[chunk[k]])
        got = jnp.concatenate([xrec[chunk[k] * SOURCES + s] for s in range(SOURCES)], axis=0)
        xall[all_rows(k), lanes(tp)] = mm(pack_ref[...], got).astype(BF16)
        for j in far_first:
            for h in range(2):
                ag1(k, h, j).start()

    def gather_more(k):
        arrived(xall.at[all_rows(k), pl.ds(0, (SIDE - 1) * LANE)], ag1_r.at[k])
        for turn in range(2):
            for h in range(2):
                for s in range(2):
                    for i in pieces(h):
                        ag2(k, h, s, (s + turn) % 2, i, second_at[h]).start()

    def gather_relay(k):
        for h in range(2):
            for s in range(2):
                arrived(xall.at[rows(k, h), pl.ds(0, PAIR)], ag2_r.at[k, h, s])
                for i in pieces(h):
                    ag2_relay(k, h, s, i, second_at[h] + behind(s)).start()

    def experts(k):
        arrived(xall.at[all_rows(k), pl.ds(0, 4 * PAIR)], ag2_rest.at[k])
        block = xall[all_rows(k), :]
        gated = jnp.minimum(mm(block, gate_ref[...]), CLAMP_LIMIT)
        clipped = jnp.clip(mm(block, up_ref[...]), -CLAMP_LIMIT, CLAMP_LIMIT)
        active = ((clipped + 1.0) * gated * jax.nn.sigmoid(GATE_SLOPE * gated)).astype(BF16)
        ypart[all_rows(k), :] = mm(active, down_ref[...]).astype(BF16)
        for kind in range(2):
            for h in range(2):
                for s in range(2):
                    for i in pieces(h):
                        rs1_raw(k, h, s, kind, i).start()

    def sum_relay(k):
        for h in range(2):
            for s in range(2):
                arrived(rs1.at[k, h, 0, s], r1_r.at[k, h, s])
                own = share_of(k, h, second_at[h] + ahead(s), s)
                comb[k, h, s] = (own + rs1[k, h, 0, s].astype(F32)).astype(BF16)
                rs1_comb(k, h, s).start()

    def sum_open(k):
        for h in range(2):
            arrived(rs1.at[k, h, pl.ds(1, 2)], r1_rest.at[k, h])
            for half in range(2):
                own = share_of(k, h, second_at[h], half)
                total = own + rs1[k, h, 2, half].astype(F32) + rs1[k, h, 1, 1 - half].astype(F32)
                band[k, h, :, half * PAIR : (half + 1) * PAIR] = total.astype(BF16)
            for j in far_first:
                rs2_copy(k, h, j).start()

    def sum_close(k):
        halves = []
        arrived(rs2.at[k], r2_r.at[k])
        for h in range(2):
            total = band[k, h, :, lanes(first_at[h])].astype(F32)
            for j in (1, 2, 3):
                total = total + rs2[k, h, j - 1].astype(F32)
            halves.append(total)
        total = jnp.concatenate(halves, axis=0).astype(BF16)
        result = mm(unpack_ref[...], total).astype(BF16)
        for s in range(SOURCES):
            rsend[chunk[k] * SOURCES + s] = result[s * SLAB : (s + 1) * SLAB]
        for i in others(k):
            give_back(k, i).start()
        if k == 0:
            rrec[ep] = rsend[ep]

    for copy in local[8:]:
        copy.wait()
    attend_open()
    gather_open(0)
    ring_open()
    gather_more(0)
    gather_open(1)
    ring_step(1)
    gather_open(2)
    gather_open(3)
    gather_relay(0)
    gather_more(1)
    ring_step(2)
    gather_more(2)
    experts(0)
    gather_more(3)
    attend_pair()
    ring_step(3)
    gather_relay(1)
    gather_relay(2)
    ring_step(4)
    gather_relay(3)
    sum_relay(0)
    attend_plus(1)
    attend_minus(1)
    ring_step(5)
    experts(1)
    experts(2)
    sum_open(0)
    ring_step(6)
    sum_relay(1)
    attend_plus(3)
    experts(3)
    ring_step(7)
    attend_minus(3)
    sum_open(1)
    sum_relay(2)
    sum_close(0)
    ring_step(8)
    sum_relay(3)
    attend_plus(5)
    attend_minus(5)
    sum_open(2)
    sum_close(1)
    attend_plus(7)
    attend_last()
    sum_open(3)
    attend_close()
    sum_close(2)

    places = jnp.transpose(place).astype(BF16)
    slots = jnp.abs(mm(places, spread_ref[...], NT)) < 0.5
    parts = []
    rest = jnp.transpose(weight)
    for _ in range(3):
        part = rest.astype(BF16)
        rest = rest - part.astype(F32)
        parts.append(jnp.where(slots, mm(part, spread_ref[...], NT), 0.0).astype(BF16))

    sum_close(3)
    share_sum()

    left(xsend.at[pl.ds(0, EP - 1)], 0)
    left(xall.at[pl.ds(0, TILE), pl.ds(0, 12 * LANE)], 1)
    left(xall.at[:, pl.ds(0, 12 * LANE)], 2)
    left(ypart.at[:, pl.ds(0, 12 * LANE)], 3)
    left(ypart.at[pl.ds(0, TILE), pl.ds(0, 12 * LANE)], 4)

    for d in range(8):
        @pl.when((z < CHIPS - 1) & (z - d >= 0))
        def _():
            plus(d).wait_send()
    for d in range(7):
        @pl.when((z + d) % CHIPS <= FAR)
        def _():
            minus(d).wait_send()

    def drain_sibling(origin, carry):
        sibling(origin).wait_send()
        return carry

    lax.fori_loop(0, z + (1 - core), drain_sibling, 0)

    arrived(pc, p_r.at[1])
    for h in range(2):
        total = pb[h, first_at[h]].astype(F32)
        for j in (1, 2, 3):
            total = total + pc[h, j - 1].astype(F32)
        rows_ref[:, h * (D // 2) : (h + 1) * (D // 2)] = total.astype(BF16)

    arrived(rrec.at[pl.ds(0, EP - 1)], b_r.at[0])
    back = jnp.concatenate([rrec[e] for e in range(EP)], axis=0)
    combined = mm(parts[2], back) + mm(parts[1], back) + mm(parts[0], back)
    experts_ref[...] = combined.astype(BF16)
    left(rsend.at[pl.ds(0, EP - 1)], 5)
    left(pa, 6)
    left(pc, 7)


def body(
    query_maps, key_maps, value_rows, head_lambda, head_gain, out_weight, token_rows, norm_gain, expert_ids,
    route_weights, gate_weight, up_weight, down_weight,
):
    spread, pack, unpack = (jnp.asarray(a, BF16) for a in slot_tables())
    vmem = pl.BlockSpec(memory_space=pltpu.VMEM)
    hbm = pl.BlockSpec(memory_space=pl.ANY)
    dma = pltpu.SemaphoreType.DMA
    return pl.pallas_call(
        kernel,
        name="layer",
        out_shape=(jax.ShapeDtypeStruct((TOK // TP, D), BF16), jax.ShapeDtypeStruct((TOK, LANE), BF16)),
        in_specs=[hbm] * 16,
        out_specs=(vmem, vmem),
        scratch_shapes=[
            pltpu.VMEM((TOK, LANE), BF16),
            pltpu.VMEM((1, 1), F32),
            pltpu.VMEM((1, LANE), F32),
            pltpu.VMEM((LANE, D), BF16),
            pltpu.VMEM((TOK, D), BF16),
            pltpu.VMEM((1, D), F32),
            pltpu.VMEM((4, TOK), jnp.int32),
            pltpu.VMEM((4, TOK), F32),
            pltpu.VMEM((PADDED, LANE), BF16),
            pltpu.VMEM((TILE, PADDED_TILE), BF16),
            pltpu.VMEM((PADDED_TILE, TILE), BF16),
            pltpu.VMEM((D, UNITS), BF16),
            pltpu.VMEM((D, UNITS), BF16),
            pltpu.VMEM((UNITS, D), BF16),
            pltpu.VMEM((EP, 2, TOK, LANE), BF16),
            pltpu.VMEM((2 * TOK, LANE), F32),
            pltpu.VMEM((2 * TOK, LANE), F32),
            pltpu.VMEM((2 * TOK, LANE), F32),
            pltpu.VMEM((2, SIDE, 32, D // 2), BF16),
            pltpu.VMEM((2, SIDE - 1, 32, D // 2), BF16),
            pltpu.VMEM((2, SIDE, 8, D // 2), BF16),
            pltpu.VMEM((2, SIDE - 1, 8, D // 2), BF16),
            pltpu.VMEM((EP, SLAB, LANE), BF16),
            pltpu.VMEM((EP, SLAB, LANE), BF16),
            pltpu.VMEM((ROWS, D), BF16),
            pltpu.VMEM((ROWS, D), BF16),
            pltpu.VMEM((STEPS, 2, 3, 2, HALF, PAIR), BF16),
            pltpu.VMEM((STEPS, 2, 2, HALF, PAIR), BF16),
            pltpu.VMEM((STEPS, 2, HALF, BAND), BF16),
            pltpu.VMEM((STEPS, 2, SIDE - 1, HALF, LANE), BF16),
            pltpu.VMEM((EP, SLAB, LANE), BF16),
            pltpu.VMEM((EP, SLAB, LANE), BF16),
            dma((16,)),
            dma((8,)), dma((9,)), dma((7,)), dma((8,)), dma((CHIPS,)), dma((CHIPS,)),
            dma((8,)), dma((2,)), dma((STEPS,)), dma((STEPS,)), dma((STEPS, 2, 2)), dma((STEPS,)), dma((STEPS, 2, 2)),
            dma((STEPS, 2)), dma((STEPS,)), dma((1,)),
        ],
        compiler_params=pltpu.CompilerParams(
            collective_id=0, has_side_effects=True, vmem_limit_bytes=60 * 1024 * 1024
        ),
    )(
        query_maps.reshape(TOK, LANE), key_maps.reshape(TOK, LANE), value_rows.reshape(TOK, LANE),
        head_lambda.reshape(1, 1), head_gain.reshape(1, LANE), out_weight, token_rows, norm_gain.reshape(1, D),
        expert_ids.T, route_weights.T, spread, pack, unpack,
        gate_weight.reshape(D, UNITS), up_weight.reshape(D, UNITS), down_weight.reshape(UNITS, D),
    )


def solution(mesh):
    placed = (
        P("ep", "tp", None), P("ep", "tp", None), P("ep", "tp", None), P("tp"), P(), P("tp", None), P("ep", None),
        P(), P("ep", None), P("ep", None), P("ep", None, "tp"), P("ep", None, "tp"), P("ep", "tp", None),
    )
    return jax.shard_map(
        body, mesh=mesh, in_specs=placed, out_specs=(P(("ep", "tp"), None), P("ep", "tp")), check_vma=False
    )
```

```python
import functools

import jax
import jax.numpy as jnp
import numpy as np
from jax import lax
from jax.experimental import pallas as pl
from jax.experimental.pallas import tpu as pltpu
from jax.sharding import PartitionSpec as P

NORM_EPS = 1e-05
CLAMP_LIMIT = 7.0
GATE_SLOPE = 1.702
MESH = pl.DeviceIdType.MESH

EP, TP, SIDE, CHIPS = 32, 16, 4, 16
CAP, SLAB = 20, 24
ORDER = ((0, 1, 2, 3), (1, 0, 3, 2), (2, 0, 1, 3), (3, 0, 1, 2))
OUTWARD = ((0, 2, 1, 3), (1, 0, 2, 3), (2, 0, 1, 3), (3, 1, 0, 2))
STEPS = len(ORDER)
SOURCES = EP // STEPS
ROWS = EP * CAP
TILE, PADDED_TILE = SOURCES * CAP, SOURCES * SLAB
HALF = TILE // 2
PADDED = EP * SLAB
D, LANE, TOK, UNITS = 2048, 128, 128, 256
BAND = SIDE * LANE
PAIR = 2 * LANE
FAR = 6
EARLY = 4
F32, BF16 = jnp.float32, jnp.bfloat16
NN = (((1,), (0,)), ((), ()))
NT = (((1,), (1,)), ((), ()))


def mm(a, b, dims=NN):
    return lax.dot_general(a, b, dims, preferred_element_type=F32)


def slot_tables():
    rows = np.arange(PADDED)
    spread = np.zeros((PADDED, LANE), np.float32)
    spread[rows, rows // SLAB] = 1.0
    spread[rows, EP] = -(rows % SLAB)
    pack = np.zeros((TILE, PADDED_TILE), np.float32)
    r = np.arange(TILE)
    pack[r, r // CAP * SLAB + r % CAP] = 1.0
    return spread, pack, pack.T.copy()


def kernel(
    q_hbm, k_hbm, v_hbm, lam_ref, gain_hbm, ow_hbm, tok_hbm, ngain_hbm, ids_hbm, wts_hbm, spread_hbm, pack_hbm,
    unpack_hbm, gate_hbm, up_hbm, down_hbm,
    rows_ref, experts_ref,
    q_ref, gain_ref, ow_ref, tok_ref, ngain_ref, ids_ref, wts_ref, spread_ref, pack_ref, unpack_ref,
    gate_ref, up_ref, down_ref,
    kv, m_ref, l_ref, acc_ref, ps, pa, pb, pc, xsend, xrec, xall, ypart, rs1, comb, band, rs2, rsend, rrec,
    local_sem, plus_s, plus_r, minus_s, minus_r, sib_s, sib_r, sent, p_r, d_r, ag1_r, ag2_r, ag2_rest, r1_r, r1_rest,
    r2_r, b_r,
):
    ep = lax.axis_index("ep")
    tp = lax.axis_index("tp")
    z, core = ep // 2, ep % 2
    x, y = tp % SIDE, tp // SIDE
    sib = z * 2 + (1 - core)

    def lanes(block, width=LANE):
        return pl.ds(pl.multiple_of(block * width, width), width)

    def remote(src, dst, ssem, rsem, e, t):
        return pltpu.make_async_remote_copy(
            src_ref=src, dst_ref=dst, send_sem=ssem, recv_sem=rsem, device_id=(e, t), device_id_type=MESH
        )

    def arrived(ref, sem):
        remote(ref, ref, sent.at[0], sem, sib, tp).wait_recv()

    def left(ref, kind):
        remote(ref, ref, sent.at[kind], b_r.at[0], sib, tp).wait_send()

    def x_peer(j):
        return y * SIDE + (x + j) % SIDE

    def y_peer(j):
        return ((y + j) % SIDE) * SIDE + x

    barrier = pltpu.get_barrier_semaphore()

    def greet_ep(n, carry):
        off = (n + 1) // 2
        to = (ep + EP // 2 + off * (1 - 2 * (n % 2))) % EP
        pl.semaphore_signal(barrier, inc=1, device_id=(to, tp), device_id_type=MESH)
        return carry

    def greet_tp(i, carry):
        pl.semaphore_signal(barrier, inc=1, device_id=(ep, (tp + i) % TP), device_id_type=MESH)
        return carry

    lax.fori_loop(0, EP - 1, greet_ep, 0)
    lax.fori_loop(1, TP, greet_tp, 0)

    moves = (
        (tok_hbm, tok_ref), (ids_hbm, ids_ref), (wts_hbm, wts_ref), (ngain_hbm, ngain_ref), (spread_hbm, spread_ref),
        (q_hbm, q_ref), (k_hbm, kv.at[ep, 0]), (v_hbm, kv.at[ep, 1]), (pack_hbm, pack_ref), (unpack_hbm, unpack_ref),
        (gain_hbm, gain_ref),
        (gate_hbm, gate_ref), (up_hbm, up_ref), (down_hbm, down_ref), (ow_hbm, ow_ref),
    )
    local = [pltpu.make_async_copy(src, dst, local_sem.at[i]) for i, (src, dst) in enumerate(moves)]
    for copy in local:
        copy.start()
    for copy in local[:5]:
        copy.wait()

    tokens = tok_ref[...].astype(F32)
    scale = lax.rsqrt(jnp.mean(tokens * tokens, axis=-1, keepdims=True) + NORM_EPS)
    mine = tok_ref[:, lanes(tp)].astype(F32)
    normed = (mine * scale * ngain_ref[:, lanes(tp)]).astype(BF16)
    first = lax.broadcasted_iota(jnp.int32, (TOK, LANE), 0)
    second = lax.broadcasted_iota(jnp.int32, (TOK, LANE), 1)
    named = jnp.zeros((TOK, LANE), F32)
    weight = jnp.zeros((TOK, LANE), F32)
    for k in range(4):
        hit = ids_ref[k : k + 1, :] == first
        named = named + jnp.where(hit, 1.0, 0.0)
        weight = weight + jnp.where(hit, wts_ref[k : k + 1, :], 0.0)
    before = jnp.where(first < second, 1.0, 0.0).astype(BF16)
    rank = mm(named.astype(BF16), before)
    place = jnp.where(named > 0.5, rank, -1.0)
    place = jnp.where(first < EP, place, jnp.where(first == EP, 1.0, 0.0))
    chosen = mm(spread_ref[...], place.astype(BF16))
    chosen = jnp.where(jnp.abs(chosen) < 0.5, 1.0, 0.0).astype(BF16)
    outgoing = mm(chosen, normed).astype(BF16)
    for e in range(EP):
        xsend[e] = outgoing[e * SLAB : (e + 1) * SLAB]
    for copy in local[5:8]:
        copy.wait()

    pl.semaphore_wait(barrier, EP - 1 + TP - 1)

    quarter = z // (CHIPS // STEPS)

    def pick(table, n):
        at = [row[n] for row in table]
        reached = [(quarter + STEPS - i) // STEPS for i in range(1, STEPS)]
        return at[0] + sum((at[i] - at[i - 1]) * reached[i - 1] for i in range(1, STEPS))

    chunk = [pick(ORDER, k) for k in range(STEPS)]
    outward = [pick(OUTWARD, n) for n in range(STEPS)]

    def others(n):
        return range(1 if n == 0 else 0, SOURCES)

    def dispatch(n, i):
        to = outward[n] * SOURCES + (ep + i) % SOURCES
        return remote(xsend.at[to], xrec.at[ep], sent.at[0], d_r.at[quarter], to, tp)

    for n in range(STEPS):
        for i in others(n):
            dispatch(n, i).start()
    xrec[ep] = xsend[ep]

    def plus(d):
        block = 2 * (z - d) + core
        return remote(kv.at[block], kv.at[block], plus_s.at[d], plus_r.at[d + 1], (ep + 2) % EP, tp)

    def plus_in(d):
        block = 2 * (z - d) + core
        return remote(kv.at[block], kv.at[block], plus_s.at[d - 1], plus_r.at[d], (ep + 2) % EP, tp)

    def minus(d):
        block = 2 * ((z + d) % CHIPS) + core
        return remote(kv.at[block], kv.at[block], minus_s.at[d], minus_r.at[d + 1], (ep + EP - 2) % EP, tp)

    def minus_in(d):
        block = 2 * ((z + d) % CHIPS) + core
        return remote(kv.at[block], kv.at[block], minus_s.at[d - 1], minus_r.at[d], (ep + EP - 2) % EP, tp)

    def sibling(origin):
        block = 2 * origin + core
        return remote(kv.at[block], kv.at[block], sib_s.at[origin], sib_r.at[origin], sib, tp)

    def sibling_in(origin):
        block = 2 * origin + 1 - core
        return remote(kv.at[block], kv.at[block], sib_s.at[origin], sib_r.at[origin], sib, tp)

    def ring_open():
        @pl.when(z < CHIPS - 1)
        def _():
            plus(0).start()

        @pl.when(z <= FAR)
        def _():
            minus(0).start()

        @pl.when(core == 0)
        def _():
            sibling(z).start()

    def ring_step(d):
        @pl.when(z - d >= 0)
        def _():
            plus_in(d).wait_recv()
            if d < 8:
                @pl.when(z < CHIPS - 1)
                def _():
                    plus(d).start()
            sibling(z - d).start()

        if d <= 7:
            origin = (z + d) % CHIPS

            @pl.when(origin <= FAR)
            def _():
                minus_in(d).wait_recv()
                if d < 7:
                    minus(d).start()

                @pl.when(origin < z)
                def _():
                    sibling(origin).start()

    far_first = (2, 1, 3)

    queries_of = []

    def attend(blocks):
        keys = jnp.concatenate([kv[b, 0] for b in blocks], axis=0)
        values = jnp.concatenate([kv[b, 1] for b in blocks], axis=0)
        scores = mm(queries_of[0], keys, NT)
        old = m_ref[:, 0:1]
        new = jnp.maximum(old, jnp.max(scores, axis=-1, keepdims=True))
        shrink = jnp.exp(old - new)
        terms = jnp.exp(scores - new)
        m_ref[...] = jnp.broadcast_to(new, (2 * TOK, LANE))
        l_ref[...] = l_ref[...] * shrink + jnp.sum(terms, axis=-1, keepdims=True)
        acc_ref[...] = acc_ref[...] * shrink + mm(terms.astype(BF16), values)

    def attend_open():
        query = q_ref[...] * jnp.asarray(0.125, BF16)
        nothing = jnp.zeros_like(query)
        queries = jnp.concatenate([jnp.where(second < 64, query, nothing), jnp.where(second < 64, nothing, query)], axis=0)
        queries_of.append(queries)
        causal = jnp.concatenate([second <= first, second <= first], axis=0)
        scores = jnp.where(causal, mm(queries, kv[ep, 0], NT), -jnp.inf)
        top_score = jnp.max(scores, axis=-1, keepdims=True)
        terms = jnp.exp(scores - top_score)
        m_ref[...] = jnp.broadcast_to(top_score, (2 * TOK, LANE))
        l_ref[...] = jnp.broadcast_to(jnp.sum(terms, axis=-1, keepdims=True), (2 * TOK, LANE))
        acc_ref[...] = mm(terms.astype(BF16), kv[ep, 1])

    def attend_pair():
        @pl.when(core == 1)
        def _():
            sibling_in(z).wait_recv()
            attend([2 * z])

    def attend_some(a, a_in, b, b_in):
        def both():
            sibling_in(a).wait_recv()
            sibling_in(b).wait_recv()
            attend([2 * a, 2 * a + 1, 2 * b, 2 * b + 1])

        def one():
            sibling_in(a).wait_recv()
            attend([2 * a, 2 * a + 1])

        pl.when(a_in & b_in)(both)
        pl.when(a_in & jnp.logical_not(b_in))(one)

    def attend_plus(d):
        attend_some(z - d, z - d >= 0, z - d - 1, z - d - 1 >= 0)

    def attend_minus(d):
        late, early = (z + d + 1) % CHIPS, (z + d) % CHIPS
        attend_some(late, z + d + 1 >= CHIPS, early, z + d >= CHIPS)

    def attend_last():
        origin = (z + 7) % CHIPS

        @pl.when(z + 7 >= CHIPS)
        def _():
            sibling_in(origin).wait_recv()
            attend([2 * origin, 2 * origin + 1])

    def attend_close():
        ratio = acc_ref[...] / l_ref[...]
        attended = ratio[:TOK] - lam_ref[0] * ratio[TOK:]
        square = jnp.mean(attended * attended, axis=-1, keepdims=True)
        head = (attended * lax.rsqrt(square + NORM_EPS) * gain_ref[...]).astype(BF16)
        product = mm(head, ow_ref[...])
        for q in range(SIDE):
            ps[0, q] = product[q * 32 : (q + 1) * 32, : D // 2].astype(BF16)
            picked = [product[(n * SIDE + q) * 8 : (n * SIDE + q) * 8 + 8, D // 2 :] for n in range(SIDE)]
            ps[1, q] = jnp.concatenate(picked, axis=0).astype(BF16)
        for j in far_first:
            for h in range(2):
                share_first(h, j).start()

    def share_first(h, j):
        to = (second_at[h] + j) % SIDE
        return remote(ps.at[h, to], pa.at[h, j - 1], sent.at[6], p_r.at[0], ep, along(h, j))

    def share_second(h, j):
        to = (first_at[h] + j) % SIDE
        return remote(pb.at[h, to], pc.at[h, j - 1], sent.at[7], p_r.at[1], ep, across(h, j))

    def share_sum():
        arrived(pa, p_r.at[0])
        for h in range(2):
            total = ps[h, second_at[h]].astype(F32)
            for j in (1, 2, 3):
                total = total + pa[h, j - 1].astype(F32)
            for n in range(SIDE):
                pb[h, n] = total[n * 8 : (n + 1) * 8].astype(BF16)
            for j in far_first:
                share_second(h, j).start()

    first_at = (x, y)
    second_at = (y, x)
    own_block = (tp, x * SIDE + y)
    turned = [(n % SIDE) * SIDE + n // SIDE for n in range(TP)]

    def rows(k, h):
        return pl.ds(pl.multiple_of(chunk[k] * TILE + h * HALF, HALF), HALF)

    def all_rows(k):
        return pl.ds(pl.multiple_of(chunk[k] * TILE, TILE), TILE)

    def ag1(k, h, j):
        part = xall.at[rows(k, h), lanes(own_block[h])]
        return remote(part, part, sent.at[1], ag1_r.at[k], ep, x_peer(j) if h == 0 else y_peer(j))


    def along(h, j):
        return y_peer(j) if h == 0 else x_peer(j)

    def across(h, j):
        return x_peer(j) if h == 0 else y_peer(j)

    def columns(q, half):
        return lanes(2 * (q % SIDE) + half, PAIR)

    def ahead(s):
        return 1 if s == 0 else SIDE - 1

    def behind(s):
        return SIDE - ahead(s)

    def ag2(k, h, s, half, q):
        part = xall.at[rows(k, h), columns(q, half)]
        sem = ag2_r.at[k, h, s] if half == s else ag2_rest.at[k]
        return remote(part, part, sent.at[2], sem, ep, along(h, ahead(s)))

    def ag2_relay(k, h, s, q):
        part = xall.at[rows(k, h), columns(q, s)]
        return remote(part, part, sent.at[2], ag2_rest.at[k], ep, along(h, ahead(s)))

    def rs1_raw(k, h, s, kind):
        q, half = (second_at[h] + 2, s) if kind == 0 else (second_at[h] + ahead(s), 1 - s)
        part = ypart.at[rows(k, h), columns(q, half)]
        sem = r1_r.at[k, h, s] if kind == 0 else r1_rest.at[k, h]
        return remote(part, rs1.at[k, h, kind, s], sent.at[3], sem, ep, along(h, ahead(s)))

    def rs1_comb(k, h, s):
        return remote(comb.at[k, h, s], rs1.at[k, h, 2, s], sent.at[3], r1_rest.at[k, h], ep, along(h, ahead(s)))

    def share_of(k, h, q, half):
        return ypart[rows(k, h), columns(q, half)].astype(F32)

    def rs2_copy(k, h, j):
        part = band.at[k, h, :, lanes((first_at[h] + j) % SIDE)]
        return remote(part, rs2.at[k, h, j - 1], sent.at[4], r2_r.at[k], ep, across(h, j))

    def give_back(k, i):
        to = chunk[k] * SOURCES + (ep + i) % SOURCES
        return remote(rsend.at[to], rrec.at[ep], sent.at[5], b_r.at[0], to, tp)

    def gather_open(k):
        arrived(xrec.at[pl.ds(chunk[k] * SOURCES, len(others(k)))], d_r.at[chunk[k]])
        got = jnp.concatenate([xrec[chunk[k] * SOURCES + s] for s in range(SOURCES)], axis=0)
        packed = mm(pack_ref[...], got).astype(BF16)
        for h in range(2):
            xall[rows(k, h), lanes(own_block[h])] = packed[h * HALF : (h + 1) * HALF]
        for j in far_first:
            for h in range(2):
                ag1(k, h, j).start()

    def gather_more(k):
        arrived(xall.at[all_rows(k), pl.ds(0, (SIDE - 1) * LANE)], ag1_r.at[k])
        for turn in range(2):
            for h in range(2):
                for s in range(2):
                    ag2(k, h, s, (s + turn) % 2, second_at[h]).start()

    def gather_relay(k):
        for h in range(2):
            for s in range(2):
                arrived(xall.at[rows(k, h), pl.ds(0, PAIR)], ag2_r.at[k, h, s])
                ag2_relay(k, h, s, second_at[h] + behind(s)).start()

    def experts(k):
        arrived(xall.at[all_rows(k), pl.ds(0, 4 * PAIR)], ag2_rest.at[k])
        lower = jnp.concatenate([xall[rows(k, 1), n * LANE : (n + 1) * LANE] for n in turned], axis=1)
        block = jnp.concatenate([xall[rows(k, 0), :], lower], axis=0)
        gated = jnp.minimum(mm(block, gate_ref[...]), CLAMP_LIMIT)
        clipped = jnp.clip(mm(block, up_ref[...]), -CLAMP_LIMIT, CLAMP_LIMIT)
        active = ((clipped + 1.0) * gated * jax.nn.sigmoid(GATE_SLOPE * gated)).astype(BF16)
        result = mm(active, down_ref[...]).astype(BF16)
        ypart[rows(k, 0), :] = result[:HALF]
        for n in range(TP):
            ypart[rows(k, 1), turned[n] * LANE : (turned[n] + 1) * LANE] = result[HALF:, n * LANE : (n + 1) * LANE]
        for kind in range(2):
            for h in range(2):
                for s in range(2):
                    rs1_raw(k, h, s, kind).start()

    def sum_relay(k):
        for h in range(2):
            for s in range(2):
                arrived(rs1.at[k, h, 0, s], r1_r.at[k, h, s])
                own = share_of(k, h, second_at[h] + ahead(s), s)
                comb[k, h, s] = (own + rs1[k, h, 0, s].astype(F32)).astype(BF16)
                rs1_comb(k, h, s).start()

    def sum_open(k):
        for h in range(2):
            arrived(rs1.at[k, h, pl.ds(1, 2)], r1_rest.at[k, h])
            for half in range(2):
                own = share_of(k, h, second_at[h], half)
                total = own + rs1[k, h, 2, half].astype(F32) + rs1[k, h, 1, 1 - half].astype(F32)
                band[k, h, :, half * PAIR : (half + 1) * PAIR] = total.astype(BF16)
            for j in far_first:
                rs2_copy(k, h, j).start()

    def sum_close(k):
        halves = []
        arrived(rs2.at[k], r2_r.at[k])
        for h in range(2):
            total = band[k, h, :, lanes(first_at[h])].astype(F32)
            for j in (1, 2, 3):
                total = total + rs2[k, h, j - 1].astype(F32)
            halves.append(total)
        total = jnp.concatenate(halves, axis=0).astype(BF16)
        result = mm(unpack_ref[...], total).astype(BF16)
        for s in range(SOURCES):
            rsend[chunk[k] * SOURCES + s] = result[s * SLAB : (s + 1) * SLAB]
        for i in others(k):
            give_back(k, i).start()
        if k == 0:
            rrec[ep] = rsend[ep]

    for copy in local[8:]:
        copy.wait()
    attend_open()
    gather_open(0)
    ring_open()
    gather_more(0)
    gather_open(1)
    ring_step(1)
    gather_open(2)
    gather_open(3)
    gather_relay(0)
    gather_more(1)
    ring_step(2)
    gather_more(2)
    experts(0)
    gather_more(3)
    attend_pair()
    ring_step(3)
    gather_relay(1)
    gather_relay(2)
    ring_step(4)
    gather_relay(3)
    sum_relay(0)
    attend_plus(1)
    attend_minus(1)
    ring_step(5)
    experts(1)
    experts(2)
    sum_open(0)
    ring_step(6)
    sum_relay(1)
    attend_plus(3)
    experts(3)
    sum_relay(2)
    pl.when(z < EARLY)(attend_close)
    ring_step(7)
    attend_minus(3)
    sum_open(1)
    sum_close(0)
    sum_relay(3)
    ring_step(8)
    attend_plus(5)
    attend_minus(5)
    sum_open(2)
    sum_close(1)
    attend_plus(7)
    attend_last()
    sum_open(3)
    pl.when(z >= EARLY)(attend_close)
    sum_close(2)
    pl.when(z < EARLY)(share_sum)

    places = jnp.transpose(place).astype(BF16)
    slots = jnp.abs(mm(places, spread_ref[...], NT)) < 0.5
    parts = []
    rest = jnp.transpose(weight)
    for _ in range(3):
        part = rest.astype(BF16)
        rest = rest - part.astype(F32)
        parts.append(jnp.where(slots, mm(part, spread_ref[...], NT), 0.0).astype(BF16))

    sum_close(3)
    pl.when(z >= EARLY)(share_sum)

    left(xsend.at[pl.ds(0, EP - 1)], 0)
    left(xall.at[pl.ds(0, TILE), pl.ds(0, 12 * LANE)], 1)
    left(xall.at[:, pl.ds(0, 12 * LANE)], 2)
    left(ypart.at[:, pl.ds(0, 12 * LANE)], 3)
    left(ypart.at[pl.ds(0, TILE), pl.ds(0, 12 * LANE)], 4)

    for d in range(8):
        @pl.when((z < CHIPS - 1) & (z - d >= 0))
        def _():
            plus(d).wait_send()
    for d in range(7):
        @pl.when((z + d) % CHIPS <= FAR)
        def _():
            minus(d).wait_send()

    def drain_sibling(origin, carry):
        sibling(origin).wait_send()
        return carry

    lax.fori_loop(0, z + (1 - core), drain_sibling, 0)

    arrived(pc, p_r.at[1])
    for h in range(2):
        total = pb[h, first_at[h]].astype(F32)
        for j in (1, 2, 3):
            total = total + pc[h, j - 1].astype(F32)
        rows_ref[:, h * (D // 2) : (h + 1) * (D // 2)] = total.astype(BF16)

    arrived(rrec.at[pl.ds(0, EP - 1)], b_r.at[0])
    back = jnp.concatenate([rrec[e] for e in range(EP)], axis=0)
    combined = mm(parts[2], back) + mm(parts[1], back) + mm(parts[0], back)
    experts_ref[...] = combined.astype(BF16)
    left(rsend.at[pl.ds(0, EP - 1)], 5)
    left(pa, 6)
    left(pc, 7)


def body(
    query_maps, key_maps, value_rows, head_lambda, head_gain, out_weight, token_rows, norm_gain, expert_ids,
    route_weights, gate_weight, up_weight, down_weight,
):
    spread, pack, unpack = (jnp.asarray(a, BF16) for a in slot_tables())
    vmem = pl.BlockSpec(memory_space=pltpu.VMEM)
    hbm = pl.BlockSpec(memory_space=pl.ANY)
    dma = pltpu.SemaphoreType.DMA
    return pl.pallas_call(
        kernel,
        name="layer",
        out_shape=(jax.ShapeDtypeStruct((TOK // TP, D), BF16), jax.ShapeDtypeStruct((TOK, LANE), BF16)),
        in_specs=[hbm] * 3 + [pl.BlockSpec(memory_space=pltpu.SMEM)] + [hbm] * 12,
        out_specs=(vmem, vmem),
        scratch_shapes=[
            pltpu.VMEM((TOK, LANE), BF16),
            pltpu.VMEM((1, LANE), F32),
            pltpu.VMEM((LANE, D), BF16),
            pltpu.VMEM((TOK, D), BF16),
            pltpu.VMEM((1, D), F32),
            pltpu.VMEM((4, TOK), jnp.int32),
            pltpu.VMEM((4, TOK), F32),
            pltpu.VMEM((PADDED, LANE), BF16),
            pltpu.VMEM((TILE, PADDED_TILE), BF16),
            pltpu.VMEM((PADDED_TILE, TILE), BF16),
            pltpu.VMEM((D, UNITS), BF16),
            pltpu.VMEM((D, UNITS), BF16),
            pltpu.VMEM((UNITS, D), BF16),
            pltpu.VMEM((EP, 2, TOK, LANE), BF16),
            pltpu.VMEM((2 * TOK, LANE), F32),
            pltpu.VMEM((2 * TOK, LANE), F32),
            pltpu.VMEM((2 * TOK, LANE), F32),
            pltpu.VMEM((2, SIDE, 32, D // 2), BF16),
            pltpu.VMEM((2, SIDE - 1, 32, D // 2), BF16),
            pltpu.VMEM((2, SIDE, 8, D // 2), BF16),
            pltpu.VMEM((2, SIDE - 1, 8, D // 2), BF16),
            pltpu.VMEM((EP, SLAB, LANE), BF16),
            pltpu.VMEM((EP, SLAB, LANE), BF16),
            pltpu.VMEM((ROWS, D), BF16),
            pltpu.VMEM((ROWS, D), BF16),
            pltpu.VMEM((STEPS, 2, 3, 2, HALF, PAIR), BF16),
            pltpu.VMEM((STEPS, 2, 2, HALF, PAIR), BF16),
            pltpu.VMEM((STEPS, 2, HALF, BAND), BF16),
            pltpu.VMEM((STEPS, 2, SIDE - 1, HALF, LANE), BF16),
            pltpu.VMEM((EP, SLAB, LANE), BF16),
            pltpu.VMEM((EP, SLAB, LANE), BF16),
            dma((15,)),
            dma((8,)), dma((9,)), dma((7,)), dma((8,)), dma((CHIPS,)), dma((CHIPS,)),
            dma((8,)), dma((2,)), dma((STEPS,)), dma((STEPS,)), dma((STEPS, 2, 2)), dma((STEPS,)), dma((STEPS, 2, 2)),
            dma((STEPS, 2)), dma((STEPS,)), dma((1,)),
        ],
        compiler_params=pltpu.CompilerParams(
            collective_id=0, has_side_effects=True, vmem_limit_bytes=60 * 1024 * 1024
        ),
    )(
        query_maps.reshape(TOK, LANE), key_maps.reshape(TOK, LANE), value_rows.reshape(TOK, LANE),
        head_lambda, head_gain.reshape(1, LANE), out_weight, token_rows, norm_gain.reshape(1, D),
        expert_ids.T, route_weights.T, spread, pack, unpack,
        gate_weight.reshape(D, UNITS), up_weight.reshape(D, UNITS), down_weight.reshape(UNITS, D),
    )


def solution(mesh):
    placed = (
        P("ep", "tp", None), P("ep", "tp", None), P("ep", "tp", None), P("tp"), P(), P("tp", None), P("ep", None),
        P(), P("ep", None), P("ep", None), P("ep", None, "tp"), P("ep", None, "tp"), P("ep", "tp", None),
    )
    return jax.shard_map(
        body, mesh=mesh, in_specs=placed, out_specs=(P(("ep", "tp"), None), P("ep", "tp")), check_vma=False
    )
```

```python
import functools

import jax
import jax.numpy as jnp
import numpy as np
from jax import lax
from jax.experimental import pallas as pl
from jax.experimental.pallas import tpu as pltpu
from jax.sharding import PartitionSpec as P

NORM_EPS = 1e-05
CLAMP_LIMIT = 7.0
GATE_SLOPE = 1.702
MESH = pl.DeviceIdType.MESH

EP, TP, SIDE, CHIPS = 32, 16, 4, 16
CAP, SLAB = 20, 20
ORDER = ((0, 1, 2, 3), (1, 0, 3, 2), (2, 0, 1, 3), (3, 0, 1, 2))
OUTWARD = ((0, 2, 1, 3), (1, 0, 2, 3), (2, 0, 1, 3), (3, 1, 0, 2))
STEPS = len(ORDER)
SOURCES = EP // STEPS
ROWS = EP * CAP
TILE, PADDED_TILE = SOURCES * CAP, SOURCES * SLAB
HALF = TILE // 2
PADDED = EP * SLAB
D, LANE, TOK, UNITS = 2048, 128, 128, 256
BAND = SIDE * LANE
PAIR = 2 * LANE
FAR = 6
EARLY = 4
F32, BF16 = jnp.float32, jnp.bfloat16
NN = (((1,), (0,)), ((), ()))
NT = (((1,), (1,)), ((), ()))


def mm(a, b, dims=NN):
    return lax.dot_general(a, b, dims, preferred_element_type=F32)


def slot_tables():
    rows = np.arange(PADDED)
    spread = np.zeros((PADDED, LANE), np.float32)
    spread[rows, rows // SLAB] = 1.0
    spread[rows, EP] = -(rows % SLAB)
    return spread


def kernel(
    q_hbm, k_hbm, v_hbm, lam_ref, gain_hbm, ow_hbm, tok_hbm, ngain_hbm, ids_hbm, wts_hbm, spread_hbm,
    gate_hbm, up_hbm, down_hbm,
    rows_ref, experts_ref,
    q_ref, gain_ref, ow_ref, tok_ref, ngain_ref, ids_ref, wts_ref, spread_ref,
    gate_ref, up_ref, down_ref,
    kv, m_ref, l_ref, acc_ref, ps, pa, pb, pc, xsend, xrec, xall, ypart, rs1, comb, band, rs2, rsend, rrec,
    local_sem, plus_s, plus_r, minus_s, minus_r, sib_s, sib_r, sent, p_r, d_r, ag1_r, ag2_r, ag2_rest, r1_r, r1_rest,
    r2_r, b_r,
):
    ep = lax.axis_index("ep")
    tp = lax.axis_index("tp")
    z, core = ep // 2, ep % 2
    x, y = tp % SIDE, tp // SIDE
    sib = z * 2 + (1 - core)

    def lanes(block, width=LANE):
        return pl.ds(pl.multiple_of(block * width, width), width)

    def remote(src, dst, ssem, rsem, e, t):
        return pltpu.make_async_remote_copy(
            src_ref=src, dst_ref=dst, send_sem=ssem, recv_sem=rsem, device_id=(e, t), device_id_type=MESH
        )

    def arrived(ref, sem):
        remote(ref, ref, sent.at[0], sem, sib, tp).wait_recv()

    def left(ref, kind):
        remote(ref, ref, sent.at[kind], b_r.at[0], sib, tp).wait_send()

    def x_peer(j):
        return y * SIDE + (x + j) % SIDE

    def y_peer(j):
        return ((y + j) % SIDE) * SIDE + x

    barrier = pltpu.get_barrier_semaphore()

    def greet_ep(n, carry):
        off = (n + 1) // 2
        to = (ep + EP // 2 + off * (1 - 2 * (n % 2))) % EP
        pl.semaphore_signal(barrier, inc=1, device_id=(to, tp), device_id_type=MESH)
        return carry

    def greet_tp(i, carry):
        pl.semaphore_signal(barrier, inc=1, device_id=(ep, (tp + i) % TP), device_id_type=MESH)
        return carry

    lax.fori_loop(0, EP - 1, greet_ep, 0)
    lax.fori_loop(1, TP, greet_tp, 0)

    moves = (
        (tok_hbm, tok_ref), (ids_hbm, ids_ref), (wts_hbm, wts_ref), (ngain_hbm, ngain_ref), (spread_hbm, spread_ref),
        (q_hbm, q_ref), (k_hbm, kv.at[ep, 0]), (v_hbm, kv.at[ep, 1]),
        (gain_hbm, gain_ref),
        (gate_hbm, gate_ref), (up_hbm, up_ref), (down_hbm, down_ref), (ow_hbm, ow_ref),
    )
    local = [pltpu.make_async_copy(src, dst, local_sem.at[i]) for i, (src, dst) in enumerate(moves)]
    for copy in local:
        copy.start()
    for copy in local[:5]:
        copy.wait()

    tokens = tok_ref[...].astype(F32)
    scale = lax.rsqrt(jnp.mean(tokens * tokens, axis=-1, keepdims=True) + NORM_EPS)
    mine = tok_ref[:, lanes(tp)].astype(F32)
    normed = (mine * scale * ngain_ref[:, lanes(tp)]).astype(BF16)
    first = lax.broadcasted_iota(jnp.int32, (TOK, LANE), 0)
    second = lax.broadcasted_iota(jnp.int32, (TOK, LANE), 1)
    named = jnp.zeros((TOK, LANE), F32)
    weight = jnp.zeros((TOK, LANE), F32)
    for k in range(4):
        hit = ids_ref[k : k + 1, :] == first
        named = named + jnp.where(hit, 1.0, 0.0)
        weight = weight + jnp.where(hit, wts_ref[k : k + 1, :], 0.0)
    before = jnp.where(first < second, 1.0, 0.0).astype(BF16)
    rank = mm(named.astype(BF16), before)
    place = jnp.where(named > 0.5, rank, -1.0)
    place = jnp.where(first < EP, place, jnp.where(first == EP, 1.0, 0.0))
    chosen = mm(spread_ref[...], place.astype(BF16))
    chosen = jnp.where(jnp.abs(chosen) < 0.5, 1.0, 0.0).astype(BF16)
    outgoing = mm(chosen, normed).astype(BF16)
    for e in range(EP):
        xsend[e] = outgoing[e * SLAB : (e + 1) * SLAB]
    for copy in local[5:8]:
        copy.wait()

    pl.semaphore_wait(barrier, EP - 1 + TP - 1)

    quarter = z // (CHIPS // STEPS)

    def pick(table, n):
        at = [row[n] for row in table]
        reached = [(quarter + STEPS - i) // STEPS for i in range(1, STEPS)]
        return at[0] + sum((at[i] - at[i - 1]) * reached[i - 1] for i in range(1, STEPS))

    chunk = [pick(ORDER, k) for k in range(STEPS)]
    outward = [pick(OUTWARD, n) for n in range(STEPS)]

    def others(n):
        return range(1 if n == 0 else 0, SOURCES)

    def dispatch(n, i):
        to = outward[n] * SOURCES + (ep + i) % SOURCES
        return remote(xsend.at[to], xrec.at[ep], sent.at[0], d_r.at[quarter], to, tp)

    for n in range(STEPS):
        for i in others(n):
            dispatch(n, i).start()
    xrec[ep] = xsend[ep]

    def plus(d):
        block = 2 * (z - d) + core
        return remote(kv.at[block], kv.at[block], plus_s.at[d], plus_r.at[d + 1], (ep + 2) % EP, tp)

    def plus_in(d):
        block = 2 * (z - d) + core
        return remote(kv.at[block], kv.at[block], plus_s.at[d - 1], plus_r.at[d], (ep + 2) % EP, tp)

    def minus(d):
        block = 2 * ((z + d) % CHIPS) + core
        return remote(kv.at[block], kv.at[block], minus_s.at[d], minus_r.at[d + 1], (ep + EP - 2) % EP, tp)

    def minus_in(d):
        block = 2 * ((z + d) % CHIPS) + core
        return remote(kv.at[block], kv.at[block], minus_s.at[d - 1], minus_r.at[d], (ep + EP - 2) % EP, tp)

    def sibling(origin):
        block = 2 * origin + core
        return remote(kv.at[block], kv.at[block], sib_s.at[origin], sib_r.at[origin], sib, tp)

    def sibling_in(origin):
        block = 2 * origin + 1 - core
        return remote(kv.at[block], kv.at[block], sib_s.at[origin], sib_r.at[origin], sib, tp)

    def ring_open():
        @pl.when(z < CHIPS - 1)
        def _():
            plus(0).start()

        @pl.when(z <= FAR)
        def _():
            minus(0).start()

        @pl.when(core == 0)
        def _():
            sibling(z).start()

    def ring_step(d):
        @pl.when(z - d >= 0)
        def _():
            plus_in(d).wait_recv()
            if d < 8:
                @pl.when(z < CHIPS - 1)
                def _():
                    plus(d).start()
            sibling(z - d).start()

        if d <= 7:
            origin = (z + d) % CHIPS

            @pl.when(origin <= FAR)
            def _():
                minus_in(d).wait_recv()
                if d < 7:
                    minus(d).start()

                @pl.when(origin < z)
                def _():
                    sibling(origin).start()

    far_first = (2, 1, 3)

    queries_of = []

    def attend(blocks):
        keys = jnp.concatenate([kv[b, 0] for b in blocks], axis=0)
        values = jnp.concatenate([kv[b, 1] for b in blocks], axis=0)
        scores = mm(queries_of[0], keys, NT)
        old = m_ref[:, 0:1]
        new = jnp.maximum(old, jnp.max(scores, axis=-1, keepdims=True))
        shrink = jnp.exp(old - new)
        terms = jnp.exp(scores - new)
        m_ref[...] = jnp.broadcast_to(new, (2 * TOK, LANE))
        l_ref[...] = l_ref[...] * shrink + jnp.sum(terms, axis=-1, keepdims=True)
        acc_ref[...] = acc_ref[...] * shrink + mm(terms.astype(BF16), values)

    def attend_open():
        query = q_ref[...] * jnp.asarray(0.125, BF16)
        nothing = jnp.zeros_like(query)
        queries = jnp.concatenate([jnp.where(second < 64, query, nothing), jnp.where(second < 64, nothing, query)], axis=0)
        queries_of.append(queries)
        causal = jnp.concatenate([second <= first, second <= first], axis=0)
        scores = jnp.where(causal, mm(queries, kv[ep, 0], NT), -jnp.inf)
        top_score = jnp.max(scores, axis=-1, keepdims=True)
        terms = jnp.exp(scores - top_score)
        m_ref[...] = jnp.broadcast_to(top_score, (2 * TOK, LANE))
        l_ref[...] = jnp.broadcast_to(jnp.sum(terms, axis=-1, keepdims=True), (2 * TOK, LANE))
        acc_ref[...] = mm(terms.astype(BF16), kv[ep, 1])

    def attend_pair():
        @pl.when(core == 1)
        def _():
            sibling_in(z).wait_recv()
            attend([2 * z])

    def attend_some(a, a_in, b, b_in):
        def both():
            sibling_in(a).wait_recv()
            sibling_in(b).wait_recv()
            attend([2 * a, 2 * a + 1, 2 * b, 2 * b + 1])

        def one():
            sibling_in(a).wait_recv()
            attend([2 * a, 2 * a + 1])

        pl.when(a_in & b_in)(both)
        pl.when(a_in & jnp.logical_not(b_in))(one)

    def attend_plus(d):
        attend_some(z - d, z - d >= 0, z - d - 1, z - d - 1 >= 0)

    def attend_minus(d):
        late, early = (z + d + 1) % CHIPS, (z + d) % CHIPS
        attend_some(late, z + d + 1 >= CHIPS, early, z + d >= CHIPS)

    def attend_last():
        origin = (z + 7) % CHIPS

        @pl.when(z + 7 >= CHIPS)
        def _():
            sibling_in(origin).wait_recv()
            attend([2 * origin, 2 * origin + 1])

    def attend_close():
        ratio = acc_ref[...] / l_ref[...]
        attended = ratio[:TOK] - lam_ref[0] * ratio[TOK:]
        square = jnp.mean(attended * attended, axis=-1, keepdims=True)
        head = (attended * lax.rsqrt(square + NORM_EPS) * gain_ref[...]).astype(BF16)
        product = mm(head, ow_ref[...])
        for q in range(SIDE):
            ps[0, q] = product[q * 32 : (q + 1) * 32, : D // 2].astype(BF16)
            picked = [product[(n * SIDE + q) * 8 : (n * SIDE + q) * 8 + 8, D // 2 :] for n in range(SIDE)]
            ps[1, q] = jnp.concatenate(picked, axis=0).astype(BF16)
        for j in far_first:
            for h in range(2):
                share_first(h, j).start()

    def share_first(h, j):
        to = (second_at[h] + j) % SIDE
        return remote(ps.at[h, to], pa.at[h, j - 1], sent.at[6], p_r.at[0], ep, along(h, j))

    def share_second(h, j):
        to = (first_at[h] + j) % SIDE
        return remote(pb.at[h, to], pc.at[h, j - 1], sent.at[7], p_r.at[1], ep, across(h, j))

    def share_sum():
        arrived(pa, p_r.at[0])
        for h in range(2):
            total = ps[h, second_at[h]].astype(F32)
            for j in (1, 2, 3):
                total = total + pa[h, j - 1].astype(F32)
            for n in range(SIDE):
                pb[h, n] = total[n * 8 : (n + 1) * 8].astype(BF16)
            for j in far_first:
                share_second(h, j).start()

    first_at = (x, y)
    second_at = (y, x)
    own_block = (tp, x * SIDE + y)
    turned = [(n % SIDE) * SIDE + n // SIDE for n in range(TP)]

    def rows(k, h):
        return pl.ds(pl.multiple_of(chunk[k] * TILE + h * HALF, HALF), HALF)

    def all_rows(k):
        return pl.ds(pl.multiple_of(chunk[k] * TILE, TILE), TILE)

    def ag1(k, h, j):
        part = xall.at[rows(k, h), lanes(own_block[h])]
        return remote(part, part, sent.at[1], ag1_r.at[k], ep, x_peer(j) if h == 0 else y_peer(j))


    def along(h, j):
        return y_peer(j) if h == 0 else x_peer(j)

    def across(h, j):
        return x_peer(j) if h == 0 else y_peer(j)

    def columns(q, half):
        return lanes(2 * (q % SIDE) + half, PAIR)

    def ahead(s):
        return 1 if s == 0 else SIDE - 1

    def behind(s):
        return SIDE - ahead(s)

    def ag2(k, h, s, half, q):
        part = xall.at[rows(k, h), columns(q, half)]
        sem = ag2_r.at[k, h, s] if half == s else ag2_rest.at[k]
        return remote(part, part, sent.at[2], sem, ep, along(h, ahead(s)))

    def ag2_relay(k, h, s, q):
        part = xall.at[rows(k, h), columns(q, s)]
        return remote(part, part, sent.at[2], ag2_rest.at[k], ep, along(h, ahead(s)))

    def rs1_raw(k, h, s, kind):
        q, half = (second_at[h] + 2, s) if kind == 0 else (second_at[h] + ahead(s), 1 - s)
        part = ypart.at[rows(k, h), columns(q, half)]
        sem = r1_r.at[k, h, s] if kind == 0 else r1_rest.at[k, h]
        return remote(part, rs1.at[k, h, kind, s], sent.at[3], sem, ep, along(h, ahead(s)))

    def rs1_comb(k, h, s):
        return remote(comb.at[k, h, s], rs1.at[k, h, 2, s], sent.at[3], r1_rest.at[k, h], ep, along(h, ahead(s)))

    def share_of(k, h, q, half):
        return ypart[rows(k, h), columns(q, half)].astype(F32)

    def rs2_copy(k, h, j):
        part = band.at[k, h, :, lanes((first_at[h] + j) % SIDE)]
        return remote(part, rs2.at[k, h, j - 1], sent.at[4], r2_r.at[k], ep, across(h, j))

    def give_back(k, i):
        to = chunk[k] * SOURCES + (ep + i) % SOURCES
        return remote(rsend.at[to], rrec.at[ep], sent.at[5], b_r.at[0], to, tp)

    def gather_open(k):
        arrived(xrec.at[pl.ds(chunk[k] * SOURCES, len(others(k)))], d_r.at[chunk[k]])
        got = jnp.concatenate([xrec[chunk[k] * SOURCES + s] for s in range(SOURCES)], axis=0)
        for h in range(2):
            xall[rows(k, h), lanes(own_block[h])] = got[h * HALF : (h + 1) * HALF]
        for j in far_first:
            for h in range(2):
                ag1(k, h, j).start()

    def gather_more(k):
        arrived(xall.at[all_rows(k), pl.ds(0, (SIDE - 1) * LANE)], ag1_r.at[k])
        for turn in range(2):
            for h in range(2):
                for s in range(2):
                    ag2(k, h, s, (s + turn) % 2, second_at[h]).start()

    def gather_relay(k):
        for h in range(2):
            for s in range(2):
                arrived(xall.at[rows(k, h), pl.ds(0, PAIR)], ag2_r.at[k, h, s])
                ag2_relay(k, h, s, second_at[h] + behind(s)).start()

    def experts(k):
        arrived(xall.at[all_rows(k), pl.ds(0, 4 * PAIR)], ag2_rest.at[k])
        lower = jnp.concatenate([xall[rows(k, 1), n * LANE : (n + 1) * LANE] for n in turned], axis=1)
        block = jnp.concatenate([xall[rows(k, 0), :], lower], axis=0)
        gated = jnp.minimum(mm(block, gate_ref[...]), CLAMP_LIMIT)
        clipped = jnp.clip(mm(block, up_ref[...]), -CLAMP_LIMIT, CLAMP_LIMIT)
        active = ((clipped + 1.0) * gated * jax.nn.sigmoid(GATE_SLOPE * gated)).astype(BF16)
        result = mm(active, down_ref[...]).astype(BF16)
        ypart[rows(k, 0), :] = result[:HALF]
        for n in range(TP):
            ypart[rows(k, 1), turned[n] * LANE : (turned[n] + 1) * LANE] = result[HALF:, n * LANE : (n + 1) * LANE]
        for kind in range(2):
            for h in range(2):
                for s in range(2):
                    rs1_raw(k, h, s, kind).start()

    def sum_relay(k):
        for h in range(2):
            for s in range(2):
                arrived(rs1.at[k, h, 0, s], r1_r.at[k, h, s])
                own = share_of(k, h, second_at[h] + ahead(s), s)
                comb[k, h, s] = (own + rs1[k, h, 0, s].astype(F32)).astype(BF16)
                rs1_comb(k, h, s).start()

    def sum_open(k):
        for h in range(2):
            arrived(rs1.at[k, h, pl.ds(1, 2)], r1_rest.at[k, h])
            for half in range(2):
                own = share_of(k, h, second_at[h], half)
                total = own + rs1[k, h, 2, half].astype(F32) + rs1[k, h, 1, 1 - half].astype(F32)
                band[k, h, :, half * PAIR : (half + 1) * PAIR] = total.astype(BF16)
            for j in far_first:
                rs2_copy(k, h, j).start()

    def sum_close(k):
        halves = []
        arrived(rs2.at[k], r2_r.at[k])
        for h in range(2):
            total = band[k, h, :, lanes(first_at[h])].astype(F32)
            for j in (1, 2, 3):
                total = total + rs2[k, h, j - 1].astype(F32)
            halves.append(total)
        total = jnp.concatenate(halves, axis=0)
        for s in range(SOURCES):
            rsend[chunk[k] * SOURCES + s] = total[s * SLAB : (s + 1) * SLAB].astype(BF16)
        for i in others(k):
            give_back(k, i).start()
        if k == 0:
            rrec[ep] = rsend[ep]

    for copy in local[8:]:
        copy.wait()
    attend_open()
    gather_open(0)
    ring_open()
    gather_more(0)
    gather_open(1)
    ring_step(1)
    gather_open(2)
    gather_open(3)
    gather_relay(0)
    gather_more(1)
    ring_step(2)
    gather_more(2)
    experts(0)
    gather_more(3)
    attend_pair()
    ring_step(3)
    gather_relay(1)
    gather_relay(2)
    ring_step(4)
    gather_relay(3)
    sum_relay(0)
    attend_plus(1)
    attend_minus(1)
    ring_step(5)
    experts(1)
    experts(2)
    sum_open(0)
    ring_step(6)
    sum_relay(1)
    attend_plus(3)
    experts(3)
    sum_relay(2)
    pl.when(z < EARLY)(attend_close)
    ring_step(7)
    attend_minus(3)
    sum_open(1)
    sum_close(0)
    sum_relay(3)
    ring_step(8)
    attend_plus(5)
    attend_minus(5)
    sum_open(2)
    sum_close(1)
    attend_plus(7)
    attend_last()
    sum_open(3)
    pl.when(z >= EARLY)(attend_close)
    sum_close(2)
    pl.when(z < EARLY)(share_sum)

    places = jnp.transpose(place).astype(BF16)
    slots = jnp.abs(mm(places, spread_ref[...], NT)) < 0.5
    parts = []
    rest = jnp.transpose(weight)
    for _ in range(3):
        part = rest.astype(BF16)
        rest = rest - part.astype(F32)
        parts.append(jnp.where(slots, mm(part, spread_ref[...], NT), 0.0).astype(BF16))

    sum_close(3)
    pl.when(z >= EARLY)(share_sum)

    left(xsend.at[pl.ds(0, EP - 1)], 0)
    left(xall.at[pl.ds(0, TILE), pl.ds(0, 12 * LANE)], 1)
    left(xall.at[:, pl.ds(0, 12 * LANE)], 2)
    left(ypart.at[:, pl.ds(0, 12 * LANE)], 3)
    left(ypart.at[pl.ds(0, TILE), pl.ds(0, 12 * LANE)], 4)

    for d in range(8):
        @pl.when((z < CHIPS - 1) & (z - d >= 0))
        def _():
            plus(d).wait_send()
    for d in range(7):
        @pl.when((z + d) % CHIPS <= FAR)
        def _():
            minus(d).wait_send()

    def drain_sibling(origin, carry):
        sibling(origin).wait_send()
        return carry

    lax.fori_loop(0, z + (1 - core), drain_sibling, 0)

    arrived(pc, p_r.at[1])
    for h in range(2):
        total = pb[h, first_at[h]].astype(F32)
        for j in (1, 2, 3):
            total = total + pc[h, j - 1].astype(F32)
        rows_ref[:, h * (D // 2) : (h + 1) * (D // 2)] = total.astype(BF16)

    arrived(rrec.at[pl.ds(0, EP - 1)], b_r.at[0])
    back = jnp.concatenate([rrec[e] for e in range(EP)], axis=0)
    combined = mm(parts[2], back) + mm(parts[1], back) + mm(parts[0], back)
    experts_ref[...] = combined.astype(BF16)
    left(rsend.at[pl.ds(0, EP - 1)], 5)
    left(pa, 6)
    left(pc, 7)


def body(
    query_maps, key_maps, value_rows, head_lambda, head_gain, out_weight, token_rows, norm_gain, expert_ids,
    route_weights, gate_weight, up_weight, down_weight,
):
    spread = jnp.asarray(slot_tables(), BF16)
    vmem = pl.BlockSpec(memory_space=pltpu.VMEM)
    hbm = pl.BlockSpec(memory_space=pl.ANY)
    dma = pltpu.SemaphoreType.DMA
    return pl.pallas_call(
        kernel,
        name="layer",
        out_shape=(jax.ShapeDtypeStruct((TOK // TP, D), BF16), jax.ShapeDtypeStruct((TOK, LANE), BF16)),
        in_specs=[hbm] * 3 + [pl.BlockSpec(memory_space=pltpu.SMEM)] + [hbm] * 10,
        out_specs=(vmem, vmem),
        scratch_shapes=[
            pltpu.VMEM((TOK, LANE), BF16),
            pltpu.VMEM((1, LANE), F32),
            pltpu.VMEM((LANE, D), BF16),
            pltpu.VMEM((TOK, D), BF16),
            pltpu.VMEM((1, D), F32),
            pltpu.VMEM((4, TOK), jnp.int32),
            pltpu.VMEM((4, TOK), F32),
            pltpu.VMEM((PADDED, LANE), BF16),
            pltpu.VMEM((D, UNITS), BF16),
            pltpu.VMEM((D, UNITS), BF16),
            pltpu.VMEM((UNITS, D), BF16),
            pltpu.VMEM((EP, 2, TOK, LANE), BF16),
            pltpu.VMEM((2 * TOK, LANE), F32),
            pltpu.VMEM((2 * TOK, LANE), F32),
            pltpu.VMEM((2 * TOK, LANE), F32),
            pltpu.VMEM((2, SIDE, 32, D // 2), BF16),
            pltpu.VMEM((2, SIDE - 1, 32, D // 2), BF16),
            pltpu.VMEM((2, SIDE, 8, D // 2), BF16),
            pltpu.VMEM((2, SIDE - 1, 8, D // 2), BF16),
            pltpu.VMEM((EP, SLAB, LANE), BF16),
            pltpu.VMEM((EP, SLAB, LANE), BF16),
            pltpu.VMEM((ROWS, D), BF16),
            pltpu.VMEM((ROWS, D), BF16),
            pltpu.VMEM((STEPS, 2, 3, 2, HALF, PAIR), BF16),
            pltpu.VMEM((STEPS, 2, 2, HALF, PAIR), BF16),
            pltpu.VMEM((STEPS, 2, HALF, BAND), BF16),
            pltpu.VMEM((STEPS, 2, SIDE - 1, HALF, LANE), BF16),
            pltpu.VMEM((EP, SLAB, LANE), BF16),
            pltpu.VMEM((EP, SLAB, LANE), BF16),
            dma((13,)),
            dma((8,)), dma((9,)), dma((7,)), dma((8,)), dma((CHIPS,)), dma((CHIPS,)),
            dma((8,)), dma((2,)), dma((STEPS,)), dma((STEPS,)), dma((STEPS, 2, 2)), dma((STEPS,)), dma((STEPS, 2, 2)),
            dma((STEPS, 2)), dma((STEPS,)), dma((1,)),
        ],
        compiler_params=pltpu.CompilerParams(
            collective_id=0, has_side_effects=True, vmem_limit_bytes=60 * 1024 * 1024
        ),
    )(
        query_maps.reshape(TOK, LANE), key_maps.reshape(TOK, LANE), value_rows.reshape(TOK, LANE),
        head_lambda, head_gain.reshape(1, LANE), out_weight, token_rows, norm_gain.reshape(1, D),
        expert_ids.T, route_weights.T, spread,
        gate_weight.reshape(D, UNITS), up_weight.reshape(D, UNITS), down_weight.reshape(UNITS, D),
    )


def solution(mesh):
    placed = (
        P("ep", "tp", None), P("ep", "tp", None), P("ep", "tp", None), P("tp"), P(), P("tp", None), P("ep", None),
        P(), P("ep", None), P("ep", None), P("ep", None, "tp"), P("ep", None, "tp"), P("ep", "tp", None),
    )
    return jax.shard_map(
        body, mesh=mesh, in_specs=placed, out_specs=(P(("ep", "tp"), None), P("ep", "tp")), check_vma=False
    )
```
